512 devices in a mesh: sp: 32 (over z, core), tp: 16 (over y, x).
Axes of the slice: x: 4, y: 4, z: 16, core: 2. Of those that a mesh axis runs over, the one named last changes fastest.
Arguments:
- cotangent: bfloat16 [4096, 2048], P('sp'), may hold values from -6 to 6
- stream: bfloat16 [4096, 2048], P('sp'), may hold values from -6 to 6
- routes: int32 [4096, 2], P('sp'), may hold values from 0 to 15, all different within a row; in each aligned block of 128 rows (0 to 127, 128 to 255, ...) at most 20 rows name the same one
- route_weights: float32 [4096, 2], P('sp'), may hold values from 0.2 to 1
- gate_proj: bfloat16 [32, 2048, 2048], P('sp', None, 'tp'), may hold values from -0.125 to 0.125
- up_proj: bfloat16 [32, 2048, 2048], P('sp', None, 'tp'), may hold values from -0.125 to 0.125
- down_proj: bfloat16 [32, 2048, 2048], P('sp', 'tp'), may hold values from -0.09375 to 0.09375
- out_weight: bfloat16 [2048, 8192], P('sp', 'tp'), may hold values from -0.0625 to 0.0625
- queries: bfloat16 [4096, 4096], P('sp', 'tp'), may hold values from -6 to 6
- keys: bfloat16 [4096, 4096], P('sp', 'tp'), may hold values from -6 to 6
- values: bfloat16 [4096, 8192], P('sp', 'tp'), may hold values from -6 to 6
- decay_rate: float32 [16], P('tp'), may hold values from 0 to 1
Outputs:
- grad_gate: bfloat16 [32, 2048, 2048], P('sp', None, 'tp')
- grad_up: bfloat16 [32, 2048, 2048], P('sp', None, 'tp')
- grad_down: bfloat16 [32, 2048, 2048], P('sp', 'tp')
- grad_out_weight: float32 [2048, 8192], P('sp', 'tp')
- grad_queries: bfloat16 [4096, 4096], P('sp', 'tp')
- grad_keys: bfloat16 [4096, 4096], P('sp', 'tp')
- grad_values: bfloat16 [4096, 8192], P('sp', 'tp')
The draws below stay inside these ranges and needn't reach their ends.
Inputs may be any that keep to these rules, and one draw needn't show every extreme that they name: `routes`: each row names two different experts. In each block of 128 consecutive tokens no expert is named more than 20 times, and in some block of every draw one expert is named exactly 20 times.
All inputs are finite; a program needn't handle non-finite values.
Results may differ from the reference program's by a relative error of at most 0.006.
Values may be sent and summed in bfloat16 or wider, within the bound.
A program may use at most 128 MiB of HBM per device.

```python
import math
import jax
import jax.numpy as jnp
import numpy as np
from jax import lax

D = 2048
FF = 4096
HEADS = 16
DK = 256
DV = 512
TOP = 2
TOK_DEV = 128
EXPERTS = 16
CAP = 20
ROWS_EXP = 640
UNITS = 128
TOKENS = 4096
N_SP = 32


def draw_decay_rate(key, part):
    folded = jax.random.fold_in(key, 17)
    key_slow, key_fast, key_pick = jax.random.split(folded, 3)
    slow_rate = jnp.exp(jax.random.uniform(key_slow, (HEADS,), jnp.float32, math.log(0.2), math.log(2.0))) / TOKENS
    fast_rate = jnp.exp(jax.random.uniform(key_fast, (HEADS,), jnp.float32, math.log(0.025), math.log(0.08)))
    chosen = jax.random.uniform(key_pick, (HEADS,), jnp.float32) < 0.5
    return jnp.where(chosen, fast_rate, slow_rate).astype(jnp.float32)


def raised(values, rng, source, target, parts, factor):
    def block_of(position):
        return (jnp.arange(values.shape[position]) // (values.shape[position] // parts)).reshape((-1,) + (1,) * (values.ndim - 1 - position))

    near = jax.random.permutation(rng, parts)[block_of(target)]
    far = (block_of(target) + parts // 2) % parts
    return jnp.where((block_of(source) == near) | (block_of(source) == far), factor * values, values)


def levels(key, extent, pieces, low, largest):
    loudness = 1.0
    for dim, blocks in pieces:
        draws = jax.random.uniform(jax.random.fold_in(jax.random.fold_in(key, 6), dim), (blocks,), jnp.float32, low / len(pieces), largest / len(pieces))
        loudness = loudness * jnp.repeat(jnp.exp(draws), extent[dim] // blocks).reshape((-1,) + (1,) * (len(extent) - 1 - dim))
    return loudness


def assign_block(key, own, number, rows, number_of, top, most, lean):
    order = jax.random.permutation(key, number_of)
    heavy_load, common = portions_of(number_of, rows * top, most, lean, True), portions_of(number_of, rows * top, most, lean, False)
    places = jnp.arange(number_of)

    def named(tallies, turn):
        used = int((tallies > 0).sum())
        fixed = max(1, used // 4)
        shifted = fixed + (places - fixed + turn * (used - fixed)) % max(1, number_of - fixed)
        return jnp.zeros((number_of,), jnp.int32).at[order[jnp.where(places < fixed, places, shifted)]].set(jnp.asarray(tallies, jnp.int32))

    tallies = jnp.where(number % 4 == 0, named(heavy_load, number // 4), named(common, number - number // 4 - 1))
    mixed = jax.random.permutation(jax.random.fold_in(own, 3), number_of)
    source_of, sink = mixed[0:number_of // 2 * 2:2], mixed[1:number_of // 2 * 2:2]
    room = jnp.minimum(tallies[source_of] - 1, most - tallies[sink]) // 2
    room = jnp.where((source_of == order[0]) | (sink == order[0]) | (tallies[sink] == 0), 0, jnp.maximum(room, 0))
    shifted = jax.random.randint(jax.random.fold_in(own, 4), (number_of // 2,), 0, 1 << 20) % (room + 1)
    tallies = tallies.at[source_of].add(-shifted).at[sink].add(shifted)
    labels = jnp.searchsorted(jnp.cumsum(tallies), jnp.arange(rows * top), side="right").astype(jnp.int32)
    table = labels.reshape(top, rows).T
    table = table[jax.random.permutation(jax.random.fold_in(own, 1), rows)]
    turn = jax.random.randint(jax.random.fold_in(own, 2), (rows, 1), 0, top)
    return jnp.take_along_axis(table, (jnp.arange(top)[None, :] + turn) % top, axis=1)


def portions_of(number_of, total, limit, skew, full):
    weights = [(1 << 20) // math.isqrt(rank ** skew) + 1 for rank in range(1, number_of + 1)]
    largest = limit if full else min(limit, max(-(-total // number_of), total * weights[0] // sum(weights)))
    least = 1 if total - largest >= number_of - 1 else 0
    counts, rest = [largest] + [least] * (number_of - 1), total - largest - least * (number_of - 1)
    while rest > 0:
        movable = [i for i in range(1, number_of) if counts[i] < largest] or [i for i in range(1, number_of) if counts[i] < limit]
        whole, left = sum([weights[i] for i in movable]), rest
        for i in movable:
            extra = min(limit - counts[i], max(1, left * weights[i] // whole), rest)
            counts[i] = counts[i] + extra
            rest = rest - extra
    return np.array(counts)


def gaussian(key, shape, width, limit, cuts=(), kind=jnp.bfloat16):
    drawn = jax.random.normal(key, shape, jnp.float32) * width
    if len(cuts) > 0:
        drawn = levels(key, shape, cuts, -0.22, 0.18) * drawn
    return jnp.clip(drawn, min=-limit, max=limit).astype(kind)


def bell_draw_with(own_key, extent, spread, bound, pieces, heavy, kind=jnp.bfloat16):
    values = spread * jax.random.normal(own_key, extent, jnp.float32)
    if pieces:
        values = values * levels(own_key, extent, pieces, -0.22, 0.18)
    return jnp.clip(raised(values, jax.random.fold_in(own_key, 3), *heavy), -bound, bound).astype(kind)


def setup_inputs(seed: int = 0) -> dict:
    seeds = jax.random.split(jax.random.key(seed), 13)
    cotangent = bell_draw_with(seeds[0], (TOKENS, D), 1.0, 6.0, ((0, 32),), (0, 1, 32, 2.75))
    stream = gaussian(seeds[1], (TOKENS, D), 1.0, 6.0, ((0, 32),))
    routes_keys = jax.random.split(jax.random.fold_in(seeds[2], 1), TOKENS // TOK_DEV)
    routes_turns = jax.random.permutation(jax.random.fold_in(seeds[2], 3), TOKENS // TOK_DEV)
    routes = jax.vmap(lambda own, number: assign_block(jax.random.fold_in(seeds[2], 2), own, number, TOK_DEV, EXPERTS, TOP, CAP, 1))(routes_keys, routes_turns).reshape((TOKENS, TOP))
    route_weights = jnp.clip(0.2 + 0.8 * jax.random.uniform(seeds[3], (TOKENS, TOP), jnp.float32) ** levels(seeds[3], (TOKENS, TOP), ((0, 32),), -0.2, 0.2), 0.2, 1.0)
    gate_proj = gaussian(seeds[4], (2 * EXPERTS, D, FF // 2), D ** -0.5, 0.125, ((0, 32), (2, 16)))
    up_proj = gaussian(seeds[5], (2 * EXPERTS, D, FF // 2), D ** -0.5, 0.125, ((0, 32), (2, 16)))
    down_proj = gaussian(seeds[6], (2 * EXPERTS, FF // 2, D), FF ** -0.5, 0.09375, ((0, 32), (1, 16)))
    out_weight = gaussian(seeds[7], (D, HEADS * DV), (HEADS * DV) ** -0.5, 0.0625, ((0, 32), (1, 16)))
    queries = gaussian(seeds[8], (TOKENS, HEADS * DK), 1.0, 6.0, ((0, 32), (1, 16)))
    keys = gaussian(seeds[9], (TOKENS, HEADS * DK), 1.0, 6.0, ((0, 32), (1, 16)))
    values = gaussian(seeds[10], (TOKENS, HEADS * DV), 1.0, 6.0, ((0, 32), (1, 16)))
    decay_rate = draw_decay_rate(jax.random.fold_in(seeds[12], 71), 0)
    return dict(cotangent=cotangent, stream=stream, routes=routes, route_weights=route_weights, gate_proj=gate_proj, up_proj=up_proj, down_proj=down_proj, out_weight=out_weight, queries=queries, keys=keys, values=values, decay_rate=decay_rate)


NORM_EPS = 1.0
precise_setting = lax.Precision.HIGHEST

def silu_grad(pre_act):
    sigmoid = jax.nn.sigmoid(pre_act)
    return sigmoid * (1.0 + pre_act * (1.0 - sigmoid))

def retain(query_wide_float, key_wide_float, value_wide_float, decay_rate):
    head_count, seq_length, key_dim = query_wide_float.shape
    value_dim = value_wide_float.shape[2]
    blocks = seq_length // TOK_DEV
    local_steps = jnp.arange(TOK_DEV, dtype=jnp.float32)
    distance = local_steps[:, None] - local_steps[None, :]
    decay_mask_matrix = jnp.where(distance >= 0, jnp.exp(-decay_rate[:, None, None] * jnp.maximum(distance, 0.0)), 0.0)
    enter_decay = jnp.exp(-decay_rate[:, None] * (local_steps + 1.0))[:, :, None]
    leave_decay = jnp.exp(-decay_rate[:, None] * (TOK_DEV - 1.0 - local_steps))[:, :, None]
    block_decay = jnp.exp(-decay_rate * TOK_DEV)[:, None, None]

    def split_blocks(array):
        return array.reshape(head_count, blocks, TOK_DEV, array.shape[2]).transpose(1, 0, 2, 3)

    def advance(carry_state, inputs):
        query_tile_rows, key_tile_rows, value_block = inputs
        attention_scores = jnp.einsum('niv,nov->nio', query_tile_rows, key_tile_rows, precision=precise_setting) * decay_mask_matrix
        result = jnp.einsum('hlm,hme->hle', attention_scores, value_block, precision=precise_setting)
        result = result + enter_decay * jnp.einsum('hld,hde->hle', query_tile_rows, carry_state, precision=precise_setting)
        added = jnp.einsum('hld,hle->hde', key_tile_rows * leave_decay, value_block, precision=precise_setting)
        return (block_decay * carry_state + added, result)
    state_zero = jnp.zeros((head_count, key_dim, value_dim), jnp.float32)
    _, outputs = lax.scan(advance, state_zero, (split_blocks(query_wide_float), split_blocks(key_wide_float), split_blocks(value_wide_float)))
    return outputs.transpose(1, 0, 2, 3).reshape(head_count, seq_length, value_dim)

def normalize(retained):
    centered = retained - lax.optimization_barrier(jnp.mean(retained, axis=-1, keepdims=True))
    return centered * lax.rsqrt(lax.optimization_barrier(jnp.mean(centered * centered, axis=-1, keepdims=True)) + NORM_EPS)

def one_expert(inputs):
    cot_rows, in_rows, gate_full, up_full, down_full = inputs
    row_count = cot_rows.shape[0]
    pre_gate = jnp.dot(in_rows, gate_full, preferred_element_type=jnp.float32)
    pre_up = jnp.dot(in_rows, up_full, preferred_element_type=jnp.float32)
    active = jax.nn.silu(pre_gate)
    hidden = (active * pre_up).astype(jnp.bfloat16)
    grad_hidden = jnp.dot(cot_rows, down_full.T, preferred_element_type=jnp.float32)
    grad_pre_gate = (grad_hidden * pre_up * silu_grad(pre_gate)).astype(jnp.bfloat16)
    grad_pre_up = (grad_hidden * active).astype(jnp.bfloat16)
    grad_gate = jnp.dot(in_rows.T, grad_pre_gate, preferred_element_type=jnp.float32).astype(jnp.bfloat16)
    grad_up = jnp.dot(in_rows.T, grad_pre_up, preferred_element_type=jnp.float32).astype(jnp.bfloat16)
    grad_down = jnp.dot(hidden.T, cot_rows, preferred_element_type=jnp.float32).astype(jnp.bfloat16)
    groups = FF // UNITS
    gate_part = jnp.einsum('rgu,dgu->grd', grad_pre_gate.astype(jnp.float32).reshape(row_count, groups, UNITS), gate_full.astype(jnp.float32).reshape(D, groups, UNITS), precision=precise_setting)
    up_part = jnp.einsum('rgu,dgu->grd', grad_pre_up.astype(jnp.float32).reshape(row_count, groups, UNITS), up_full.astype(jnp.float32).reshape(D, groups, UNITS), precision=precise_setting)
    group_part = lax.optimization_barrier((gate_part + up_part).astype(jnp.bfloat16))
    grad_in = lax.optimization_barrier(jnp.sum(group_part.astype(jnp.float32), axis=0))
    return (grad_gate, grad_up, grad_down, grad_in)

def reference(cotangent, stream, routes, route_weights, gate_proj, up_proj, down_proj, out_weight, queries, keys, values, decay_rate):
    experts = N_SP // 2
    half_units = FF // 2
    assigned = TOK_DEV * TOP
    by_block = routes.reshape(N_SP, assigned)
    onehot = (by_block[:, :, None] == jnp.arange(experts, dtype=jnp.int32)[None, None, :]).astype(jnp.int32)
    slot_rank = lax.optimization_barrier(jnp.sum((jnp.cumsum(onehot, axis=1) - 1) * onehot, axis=2))
    buffer_row = (jnp.arange(N_SP, dtype=jnp.int32)[:, None] * CAP + slot_rank).reshape(-1).astype(jnp.int32)
    expert_of = by_block.reshape(-1).astype(jnp.int32)
    token_of = (jnp.arange(TOKENS * TOP, dtype=jnp.int32) // TOP).astype(jnp.int32)
    scaled = (route_weights[:, :, None] * cotangent[:, None, :].astype(jnp.float32)).reshape(TOKENS * TOP, D).astype(jnp.bfloat16)
    cot_buffer = jnp.zeros((experts, ROWS_EXP, D), jnp.bfloat16).at[expert_of, buffer_row].set(scaled)
    row_buffer = jnp.zeros((experts, ROWS_EXP, D), jnp.bfloat16).at[expert_of, buffer_row].set(stream[token_of])
    gate_full = gate_proj.reshape(experts, 2, D, half_units).transpose(0, 2, 1, 3).reshape(experts, D, FF)
    up_full = up_proj.reshape(experts, 2, D, half_units).transpose(0, 2, 1, 3).reshape(experts, D, FF)
    down_full = down_proj.reshape(experts, FF, D)
    grad_gate, grad_up, grad_down, grad_in = lax.map(one_expert, (cot_buffer, row_buffer, gate_full, up_full, down_full))
    grad_gate = grad_gate.reshape(experts, D, 2, half_units).transpose(0, 2, 1, 3).reshape(2 * experts, D, half_units)
    grad_up = grad_up.reshape(experts, D, 2, half_units).transpose(0, 2, 1, 3).reshape(2 * experts, D, half_units)
    grad_down = grad_down.reshape(2 * experts, half_units, D)
    routed_grad = lax.optimization_barrier(jnp.sum(grad_in[expert_of, buffer_row].reshape(TOKENS, TOP, D), axis=1))
    mid_grad = (cotangent.astype(jnp.float32) + routed_grad).astype(jnp.bfloat16)
    query_wide_float = queries.astype(jnp.float32).reshape(TOKENS, HEADS, DK).transpose(1, 0, 2)
    key_wide_float = keys.astype(jnp.float32).reshape(TOKENS, HEADS, DK).transpose(1, 0, 2)
    value_wide_float = values.astype(jnp.float32).reshape(TOKENS, HEADS, DV).transpose(1, 0, 2)

    def mixer(query_in, key_in, value_in):
        return normalize(retain(query_in, key_in * DK ** (-0.5), value_in, decay_rate))
    normed, pullback = jax.vjp(mixer, query_wide_float, key_wide_float, value_wide_float)
    mixed = normed.transpose(1, 0, 2).reshape(TOKENS, HEADS * DV).astype(jnp.bfloat16)
    grad_out_weight = jnp.dot(mid_grad.T, mixed, preferred_element_type=jnp.float32)
    grad_mixed = jnp.dot(mid_grad, out_weight, preferred_element_type=jnp.float32)
    query_gradient, key_gradient, grad_v = pullback(grad_mixed.reshape(TOKENS, HEADS, DV).transpose(1, 0, 2))
    grad_queries = query_gradient.transpose(1, 0, 2).reshape(TOKENS, HEADS * DK).astype(jnp.bfloat16)
    grad_keys = key_gradient.transpose(1, 0, 2).reshape(TOKENS, HEADS * DK).astype(jnp.bfloat16)
    grad_values = grad_v.transpose(1, 0, 2).reshape(TOKENS, HEADS * DV).astype(jnp.bfloat16)
    return (grad_gate, grad_up, grad_down, grad_out_weight, grad_queries, grad_keys, grad_values)
```

```python
import functools

import jax
import jax.numpy as jnp
from jax import lax
from jax.experimental import pallas as pl
from jax.experimental.pallas import tpu as pltpu
from jax.sharding import Mesh
from jax.sharding import PartitionSpec as P

SP = ("z", "c")
TP = ("y", "x")
EVERY = ("z", "c", "y", "x")
NORM_EPS = 1.0
SLOTS = 20
PAIR = 2 * SLOTS
BACK = 24
LANES = 128
BF = jnp.bfloat16
F32 = jnp.float32
MESH = pl.DeviceIdType.MESH


def dot(a, b, left=1, right=0):
    return lax.dot_general(a, b, (((left,), (right,)), ((), ())), preferred_element_type=F32)


def iota(shape, dim):
    return lax.broadcasted_iota(jnp.int32, shape, dim)


def moe_kernel(
    nz,
    routes_ref,
    weights_ref,
    cot_hbm,
    stream_hbm,
    gate_hbm,
    up_hbm,
    down_hbm,
    gg_ref,
    gu_ref,
    gd_ref,
    mid_ref,
    wcat,
    down_v,
    cot_s,
    str_s,
    sbuf,
    xs,
    acc,
    wide,
    wide_t,
    gsend,
    gown,
    gpart,
    pbuf,
    pown,
    qbuf,
    tsum,
    town,
    vbuf,
    rsend,
    ret,
    mid_s,
    loc,
    z_s,
    z_r,
    w_s,
    w_r,
    a_s,
    a_r,
    b_s,
    b_r,
    d_s,
    d_r,
    g_s,
    g_r,
    q_s,
    q_r,
    v_s,
    v_r,
    r_s,
    r_r,
    m_s,
    m_r,
):
    z, c, y, x = (lax.axis_index(a) for a in EVERY)
    rows = nz * PAIR
    half = rows // 2
    kept = nz * SLOTS
    t = y * 4 + x

    def peer(da, db):
        py = lax.rem(y + (1 - c) * da + c * db, 4)
        px = lax.rem(x + c * da + (1 - c) * db, 4)
        return (z, c, py, px)

    def tid(da, db):
        _, _, py, px = peer(da, db)
        return py * 4 + px

    def other_tid(da, db):
        py = lax.rem(y + c * da + (1 - c) * db, 4)
        px = lax.rem(x + (1 - c) * da + c * db, 4)
        return py * 4 + px

    def at_z(dz):
        return (lax.rem(z + dz, nz), c, y, x)

    partner = (z, 1 - c, y, x)

    def rc(src, dst, ss, rs, dev):
        return pltpu.make_async_remote_copy(
            src_ref=src, dst_ref=dst, send_sem=ss, recv_sem=rs, device_id=dev, device_id_type=MESH
        )

    barrier = pltpu.get_barrier_semaphore()

    @pl.loop(1, nz)
    def _(dz):
        pl.semaphore_signal(barrier, inc=1, device_id=at_z(dz), device_id_type=MESH)

    @pl.loop(1, 16)
    def _(k):
        pl.semaphore_signal(
            barrier, inc=1, device_id=peer(k // 4, lax.rem(k, 4)), device_id_type=MESH
        )

    pl.semaphore_signal(barrier, inc=1, device_id=partner, device_id_type=MESH)

    cols = pl.ds(pl.multiple_of(t * LANES, LANES), LANES)
    local = [
        pltpu.make_async_copy(cot_hbm.at[:, cols], cot_s, loc.at[0]),
        pltpu.make_async_copy(stream_hbm.at[:, cols], str_s, loc.at[1]),
        pltpu.make_async_copy(gate_hbm, wcat.at[0, :, pl.ds(0, LANES)], loc.at[2]),
        pltpu.make_async_copy(up_hbm, wcat.at[0, :, pl.ds(LANES, LANES)], loc.at[3]),
        pltpu.make_async_copy(down_hbm, down_v, loc.at[4]),
    ]
    for copy in local:
        copy.start()

    experts = iota((nz, LANES), 0)
    named = [(experts == routes_ref[k : k + 1, :]).astype(F32) for k in range(2)]
    before = (iota((LANES, LANES), 0) < iota((LANES, LANES), 1)).astype(BF)
    count = dot((named[0] + named[1]).astype(BF), before)
    rank = [
        jnp.sum(named[k] * count, axis=0, keepdims=True).astype(jnp.int32) for k in range(2)
    ]
    slot = [routes_ref[k : k + 1, :] * PAIR + rank[k] for k in range(2)]
    places = iota((rows, LANES), 0)
    acc[...] = jnp.zeros_like(acc)
    local[0].wait()
    local[1].wait()
    cot = cot_s[...].astype(F32)
    packed = dot(
        jnp.logical_or(places == slot[0] + SLOTS, places == slot[1] + SLOTS).astype(F32).astype(BF),
        str_s[...],
    )
    for k in range(2):
        scaled = (weights_ref[:, k : k + 1] * cot).astype(BF)
        packed = packed + dot((places == slot[k]).astype(F32).astype(BF), scaled)
    sbuf[...] = packed.astype(BF)

    pl.semaphore_wait(barrier, nz - 1 + 15 + 1)

    mine = pl.ds(pl.multiple_of(z * PAIR, 8), PAIR)
    for k in range(1, nz):
        dz = nz // 2 + (k // 2 if k % 2 == 0 else -(k // 2))
        there = pl.ds(pl.multiple_of(lax.rem(z + dz, nz) * PAIR, 8), PAIR)
        rc(sbuf.at[there], xs.at[c, t, mine], z_s.at[dz], z_r.at[dz], at_z(dz)).start()
    own = pltpu.make_async_copy(sbuf.at[mine], xs.at[c, t, mine], loc.at[5])
    own.start()
    local[2].wait()
    local[3].wait()
    weight_copy = rc(wcat.at[0], wcat.at[1], w_s, w_r, partner)
    weight_copy.start()
    local[4].wait()
    own.wait()
    for dz in range(1, nz):
        here = pl.ds(pl.multiple_of(lax.rem(z + nz - dz, nz) * PAIR, 8), PAIR)
        rc(sbuf.at[mine], xs.at[c, t, here], z_s.at[dz], z_r.at[dz], at_z(dz)).wait_recv()

    def product(core, piece):
        a = xs[core, piece]
        deep = pl.ds(pl.multiple_of(piece * LANES, LANES), LANES)
        acc[core, :, 0:256] += dot(a, wcat[0, deep, :])
        acc[core, :, 256:384] += dot(a, down_v[:, deep], 1, 1)

    first = pl.ds(0, half)
    last = pl.ds(half, half)

    def a_copy(k, piece):
        part = (slice(None), slice(None), first, last)[k]
        ref = xs.at[c, piece] if k < 2 else xs.at[c, piece, part]
        return rc(ref, ref, a_s.at[k], a_r.at[k], peer(1 if k % 2 == 0 else 3, 0))

    def b_copy(i, k, piece):
        part = (slice(None), slice(None), first, last)[k]
        ref = xs.at[c, piece] if k < 2 else xs.at[c, piece, part]
        return rc(ref, ref, b_s.at[i, k], b_r.at[i, k], peer(0, 1 if k % 2 == 0 else 3))

    def d_copy(i, j, core, piece):
        ref = xs.at[core, piece]
        return rc(ref, ref, d_s.at[i, j], d_r.at[i, j], partner)

    def spread(i, piece):
        b_copy(i, 0, piece).start()
        b_copy(i, 1, piece).start()
        d_copy(i, 0, c, piece).start()

    a_copy(0, t).start()
    a_copy(1, t).start()
    spread(0, t)
    product(c, t)
    piece = tid(3, 0)
    a_copy(0, piece).wait_recv()
    a_copy(2, piece).start()
    spread(1, piece)
    other = tid(1, 0)
    a_copy(1, other).wait_recv()
    a_copy(3, other).start()
    spread(2, other)
    product(c, piece)
    product(c, other)
    piece = tid(2, 0)
    a_copy(2, piece).wait_recv()
    a_copy(3, piece).wait_recv()
    spread(3, piece)
    product(c, piece)

    def offset(i):
        return (lax.rem(i + 1, 3) + 1) * jnp.minimum(i, 1)

    @pl.loop(0, 4)
    def _(i):
        da = offset(i)
        left, right, far = tid(da, 3), tid(da, 1), tid(da, 2)
        b_copy(i, 0, left).wait_recv()
        b_copy(i, 2, left).start()
        d_copy(i, 1, c, left).start()
        b_copy(i, 1, right).wait_recv()
        b_copy(i, 3, right).start()
        d_copy(i, 2, c, right).start()
        product(c, left)
        product(c, right)
        b_copy(i, 2, far).wait_recv()
        b_copy(i, 3, far).wait_recv()
        d_copy(i, 3, c, far).start()
        product(c, far)
        for j in range(4):
            piece = other_tid(da, (0, 3, 1, 2)[j])
            d_copy(i, j, 1 - c, piece).wait_recv()
            product(1 - c, piece)

    @pl.loop(0, 2 * rows // 80)
    def _(k):
        core = k // (rows // 80)
        at = pl.ds(pl.multiple_of(lax.rem(k, rows // 80) * 80, 8), 80)
        lane_row = iota((80, LANES), 0)
        is_in = jnp.logical_or(
            jnp.logical_and(lane_row >= 20, lane_row < 40), lane_row >= 60
        )
        pre_gate = acc[core, at, 0:128]
        pre_up = acc[core, at, 128:256]
        grad_hidden = pltpu.roll(acc[core, at, 256:384], 20, axis=0)
        gate = jax.nn.sigmoid(pre_gate)
        active = pre_gate * gate
        hidden = active * pre_up
        grad_gate = grad_hidden * pre_up * (gate * (1.0 + pre_gate * (1.0 - gate)))
        grad_up = grad_hidden * active
        wide[core, at, 0:128] = jnp.where(is_in, grad_gate, 0.0).astype(BF)
        wide[core, at, 128:256] = jnp.where(is_in, grad_up, 0.0).astype(BF)
        wide[core, at, 256:384] = jnp.where(is_in, 0.0, pltpu.roll(hidden, 60, axis=0)).astype(BF)

    low = iota((kept, rows), 0)
    pick = (iota((kept, rows), 1) == low + SLOTS * ((low * 3277) // 65536) + SLOTS)
    pick = pick.astype(F32).astype(BF)
    gsend[...] = dot(pick, wide[1 - c, :, 0:256]).astype(BF)
    grad_copy = rc(gsend, gpart, g_s, g_r, partner)
    grad_copy.start()
    gown[...] = dot(pick, wide[c, :, 0:256]).astype(BF)
    weight_copy.wait_recv()
    grad_copy.wait_recv()

    def partial_in(piece):
        deep = pl.ds(pl.multiple_of(piece * LANES, LANES), LANES)
        return dot(gown[...], wcat[0, deep, :], 1, 1) + dot(gpart[...], wcat[1, deep, :], 1, 1)

    def q_copy(da):
        return rc(pbuf.at[da - 1], qbuf.at[da - 1], q_s.at[da - 1], q_r.at[da - 1], peer(da, 0))

    for da in (2, 1, 3):

        @pl.loop(0, 4)
        def _(db):
            pbuf[da - 1, db] = partial_in(tid(da, db)).astype(BF)

        q_copy(da).start()

    @pl.loop(0, 4)
    def _(db):
        pown[db] = partial_in(tid(0, db))

    for core in range(2):
        wide_t[core] = wide[core].T

    @pl.loop(0, 16)
    def _(piece):
        deep = pl.ds(pl.multiple_of(piece * LANES, LANES), LANES)
        total = dot(wide_t[0], xs[0, piece]) + dot(wide_t[1], xs[1, piece])
        gd_ref[:, deep] = total[256:384].astype(BF)
        gg_ref[deep, :] = total[0:128].T.astype(BF)
        gu_ref[deep, :] = total[128:256].T.astype(BF)

    for da in (1, 3, 2):
        q_copy(da).wait_recv()

    def v_copy(db):
        return rc(tsum.at[db - 1], vbuf.at[db - 1], v_s.at[db - 1], v_r.at[db - 1], peer(0, db))

    for db in (2, 1, 3):
        whole = pown[db]
        for da in range(3):
            whole = whole + qbuf[da, db].astype(F32)
        tsum[db - 1] = whole.astype(BF)
        v_copy(db).start()
    whole = pown[0]
    for da in range(3):
        whole = whole + qbuf[da, 0].astype(F32)
    town[...] = whole
    for db in (1, 3, 2):
        v_copy(db).wait_recv()
    whole = town[...]
    for db in range(3):
        whole = whole + vbuf[db].astype(F32)
    low = iota((nz * BACK, kept), 0)
    block = (low * 2731) // 65536
    spreadm = jnp.logical_and(
        iota((nz * BACK, kept), 1) == low - (BACK - SLOTS) * block, low - BACK * block < SLOTS
    )
    rsend[...] = dot(spreadm.astype(F32).astype(BF), whole.astype(BF)).astype(BF)

    here = pl.ds(pl.multiple_of(z * BACK, 8), BACK)
    for k in range(1, nz):
        dz = nz // 2 + (k // 2 if k % 2 == 0 else -(k // 2))
        there = pl.ds(pl.multiple_of(lax.rem(z + dz, nz) * BACK, 8), BACK)
        rc(rsend.at[there], ret.at[here], r_s.at[dz], r_r.at[dz], at_z(dz)).start()
    own = pltpu.make_async_copy(rsend.at[here], ret.at[here], loc.at[6])
    own.start()
    places = iota((nz * BACK, LANES), 0)
    take = jnp.logical_or(
        places == routes_ref[0:1, :] * BACK + rank[0], places == routes_ref[1:2, :] * BACK + rank[1]
    )
    take = take.astype(F32).astype(BF)
    own.wait()
    for dz in range(1, nz):
        there = pl.ds(pl.multiple_of(lax.rem(z + nz - dz, nz) * BACK, 8), BACK)
        rc(rsend.at[here], ret.at[there], r_s.at[dz], r_r.at[dz], at_z(dz)).wait_recv()
    mid_s[:, cols] = (cot_s[...].astype(F32) + dot(take, ret[...], 0, 0)).astype(BF)

    @pl.loop(1, 16)
    def _(k):
        dev = peer(k // 4, lax.rem(k, 4))
        rc(mid_s.at[:, cols], mid_s.at[:, cols], m_s.at[k], m_r.at[k], dev).start()

    @pl.loop(1, 16)
    def _(k):
        back = tid(lax.rem(4 - k // 4, 4), lax.rem(4 - lax.rem(k, 4), 4))
        theirs = pl.ds(pl.multiple_of(back * LANES, LANES), LANES)
        dev = peer(k // 4, lax.rem(k, 4))
        rc(mid_s.at[:, cols], mid_s.at[:, theirs], m_s.at[k], m_r.at[k], dev).wait_recv()

    mid_ref[...] = mid_s[...]

    for dz in range(1, nz):
        rc(sbuf.at[mine], xs.at[c, t, mine], z_s.at[dz], z_r.at[dz], at_z(dz)).wait_send()
        rc(rsend.at[here], ret.at[here], r_s.at[dz], r_r.at[dz], at_z(dz)).wait_send()
    weight_copy.wait_send()
    grad_copy.wait_send()
    for k in range(4):
        a_copy(k, t).wait_send()

    @pl.loop(0, 4)
    def _(i):
        for k in range(4):
            b_copy(i, k, t).wait_send()
            d_copy(i, k, c, t).wait_send()

    for k in range(1, 4):
        q_copy(k).wait_send()
        v_copy(k).wait_send()

    @pl.loop(1, 16)
    def _(k):
        dev = peer(k // 4, lax.rem(k, 4))
        rc(mid_s.at[:, cols], mid_s.at[:, cols], m_s.at[k], m_r.at[k], dev).wait_send()


def moe(nz, routes, route_weights, cotangent, stream, gate, up, down):
    width = cotangent.shape[1]
    rows, kept = nz * PAIR, nz * SLOTS
    any_ = pl.BlockSpec(memory_space=pl.ANY)
    vmem = pl.BlockSpec(memory_space=pltpu.VMEM)
    dma = pltpu.SemaphoreType.DMA
    return pl.pallas_call(
        functools.partial(moe_kernel, nz),
        out_shape=(
            jax.ShapeDtypeStruct((width, LANES), BF),
            jax.ShapeDtypeStruct((width, LANES), BF),
            jax.ShapeDtypeStruct((LANES, width), BF),
            jax.ShapeDtypeStruct((LANES, width), BF),
        ),
        in_specs=[vmem, vmem, any_, any_, any_, any_, any_],
        out_specs=(vmem,) * 4,
        scratch_shapes=[
            pltpu.VMEM((2, width, 2 * LANES), BF),
            pltpu.VMEM((LANES, width), BF),
            pltpu.VMEM((LANES, LANES), BF),
            pltpu.VMEM((LANES, LANES), BF),
            pltpu.VMEM((rows, LANES), BF),
            pltpu.VMEM((2, 16, rows, LANES), BF),
            pltpu.VMEM((2, rows, 3 * LANES), F32),
            pltpu.VMEM((2, rows, 3 * LANES), BF),
            pltpu.VMEM((2, 3 * LANES, rows), BF),
            pltpu.VMEM((kept, 2 * LANES), BF),
            pltpu.VMEM((kept, 2 * LANES), BF),
            pltpu.VMEM((kept, 2 * LANES), BF),
            pltpu.VMEM((3, 4, kept, LANES), BF),
            pltpu.VMEM((4, kept, LANES), F32),
            pltpu.VMEM((3, 4, kept, LANES), BF),
            pltpu.VMEM((3, kept, LANES), BF),
            pltpu.VMEM((kept, LANES), F32),
            pltpu.VMEM((3, kept, LANES), BF),
            pltpu.VMEM((nz * BACK, LANES), BF),
            pltpu.VMEM((nz * BACK, LANES), BF),
            pltpu.VMEM((LANES, width), BF),
            dma((7,)),
            dma((nz,)),
            dma((nz,)),
            dma,
            dma,
            dma((4,)),
            dma((4,)),
            dma((4, 4)),
            dma((4, 4)),
            dma((4, 4)),
            dma((4, 4)),
            dma,
            dma,
            dma((3,)),
            dma((3,)),
            dma((3,)),
            dma((3,)),
            dma((nz,)),
            dma((nz,)),
            dma((16,)),
            dma((16,)),
        ],
        compiler_params=pltpu.CompilerParams(
            collective_id=0, has_side_effects=True, vmem_limit_bytes=56 * 2**20
        ),
        cost_estimate=pl.CostEstimate(flops=60_000_000_000, bytes_accessed=0, transcendentals=0),
        name="moe",
    )(routes.T, route_weights, cotangent, stream, gate, up, down)


def owner_scan(state, weights):
    parts = weights.shape[0]
    piece = state.astype(BF).reshape(parts, -1, state.shape[1])
    piece = lax.all_to_all(piece, SP, 0, 0, tiled=True)
    mixed = jnp.einsum(
        "bj,jxy->bxy", weights, piece.astype(F32), precision=lax.Precision.HIGHEST
    ).astype(BF)
    return lax.all_to_all(mixed, SP, 0, 0, tiled=True).reshape(state.shape)


def local(
    cotangent,
    stream,
    routes,
    route_weights,
    gate_proj,
    up_proj,
    down_proj,
    out_weight,
    queries,
    keys,
    values,
    decay_rate,
):
    nz = lax.axis_size("z")
    blocks = 2 * nz
    tok_rows = cotangent.shape[0]
    rate = decay_rate[0]
    steps = jnp.arange(tok_rows, dtype=F32)
    distance = steps[:, None] - steps[None, :]
    mask = jnp.where(distance >= 0, jnp.exp(-rate * jnp.maximum(distance, 0.0)), 0.0)
    enter = jnp.exp(-rate * (steps + 1.0))[:, None]
    leave = jnp.exp(-rate * (tok_rows - 1.0 - steps))[:, None]
    start = jnp.exp(-rate * steps)[:, None]
    trail = jnp.exp(-rate * (tok_rows - steps))[:, None]
    order = jnp.arange(blocks, dtype=F32)
    apart = order[:, None] - order[None, :] - 1.0
    earlier = jnp.where(apart >= 0, jnp.exp(-rate * tok_rows * jnp.maximum(apart, 0.0)), 0.0)
    later = earlier.T
    keys = keys * BF(keys.shape[1] ** -0.5)
    key_wide = keys.astype(F32)
    query_wide = queries.astype(F32)
    carried = owner_scan(dot((key_wide * leave).astype(BF), values, 0, 0), earlier)
    scores = dot(queries, keys, 1, 1) * mask
    scores_b = scores.astype(BF)
    retained = dot(scores_b, values) + enter * dot(queries, carried)
    centered = retained - jnp.mean(retained, axis=-1, keepdims=True)
    inv_scale = lax.rsqrt(jnp.mean(centered * centered, axis=-1, keepdims=True) + NORM_EPS)
    normed = centered * inv_scale
    mixed = normed.astype(BF)
    weight = lax.all_gather(out_weight, SP, axis=0, tiled=True)

    grad_gate, grad_up, grad_down, mid_grad = moe(
        nz, routes, route_weights, cotangent, stream, gate_proj[0], up_proj[0], down_proj[0]
    )

    head_grad = dot(mid_grad, weight)
    grad_out_weight = dot(mid_grad, mixed, 0, 0)
    for axis in SP:
        grad_out_weight = lax.psum_scatter(grad_out_weight, axis, scatter_dimension=0, tiled=True)
    grad_retained = inv_scale * (
        head_grad
        - jnp.mean(head_grad, axis=-1, keepdims=True)
        - normed * jnp.mean(head_grad * normed, axis=-1, keepdims=True)
    )
    ret_b = grad_retained.astype(BF)
    future = owner_scan(dot((query_wide * start).astype(BF), ret_b, 0, 0), later)
    score_grad = (dot(ret_b, values, 1, 1) * mask).astype(BF)
    grad_queries = dot(score_grad, keys) + enter * dot(ret_b, carried, 1, 1)
    grad_keys = (
        dot(score_grad, queries, 0, 0) + trail * dot(values, future, 1, 1)
    ) * queries.shape[1] ** (-0.5)
    grad_values = dot(scores_b, ret_b, 0, 0) + trail * dot(keys, future)
    return (
        grad_gate[None],
        grad_up[None],
        grad_down[None],
        grad_out_weight,
        grad_queries.astype(BF),
        grad_keys.astype(BF),
        grad_values.astype(BF),
    )


def solution(mesh):
    blocks, heads = mesh.devices.shape
    split = Mesh(mesh.devices.reshape(blocks // 2, 2, 4, heads // 4), EVERY)
    tokens = P(SP, None)
    tiles = P(SP, TP)
    in_specs = (
        tokens,
        tokens,
        tokens,
        tokens,
        P(SP, None, TP),
        P(SP, None, TP),
        P(SP, TP, None),
        tiles,
        tiles,
        tiles,
        tiles,
        P(TP),
    )
    out_specs = (
        P(SP, None, TP),
        P(SP, None, TP),
        P(SP, TP, None),
        tiles,
        tiles,
        tiles,
        tiles,
    )
    return jax.shard_map(local, mesh=split, in_specs=in_specs, out_specs=out_specs, check_vma=False)
```

```python
import functools

import jax
import jax.numpy as jnp
from jax import lax
from jax.experimental import pallas as pl
from jax.experimental.pallas import tpu as pltpu
from jax.sharding import Mesh
from jax.sharding import PartitionSpec as P

SP = ("z", "c")
TP = ("y", "x")
EVERY = ("z", "c", "y", "x")
NORM_EPS = 1.0
SLOTS = 20
PAIR = 2 * SLOTS
BACK = 24
LANES = 128
BF = jnp.bfloat16
F32 = jnp.float32
MESH = pl.DeviceIdType.MESH


def dot(a, b, left=1, right=0):
    return lax.dot_general(a, b, (((left,), (right,)), ((), ())), preferred_element_type=F32)


def iota(shape, dim):
    return lax.broadcasted_iota(jnp.int32, shape, dim)


def kernel(
    nz,
    routes_ref,
    weights_ref,
    cot_hbm,
    stream_hbm,
    gate_hbm,
    up_hbm,
    down_hbm,
    out_weight_hbm,
    q_ref,
    k_ref,
    v_ref,
    rate_ref,
    gg_ref,
    gu_ref,
    gd_ref,
    gow_ref,
    gq_ref,
    gk_ref,
    gv_ref,
    wcat,
    down_v,
    cot_s,
    str_s,
    sbuf,
    xs,
    acc,
    wide,
    wide_t,
    gsend,
    gown,
    gpart,
    pbuf,
    pown,
    qbuf,
    tsum,
    town,
    vbuf,
    rsend,
    ret,
    mids,
    wfull,
    state,
    half_state,
    slices,
    scanned,
    carried,
    mixes,
    scores,
    norm_s,
    inv_s,
    back_state,
    half_back,
    bslices,
    bscanned,
    future,
    prods,
    up_s,
    up_r,
    dn_s,
    dn_r,
    loc,
    z_s,
    z_r,
    w_s,
    w_r,
    a_s,
    a_r,
    b_s,
    b_r,
    d_s,
    d_r,
    g_s,
    g_r,
    q_s,
    q_r,
    v_s,
    v_r,
    r_s,
    r_r,
    m_s,
    m_r,
    wr_s,
    wr_r,
    wd_s,
    wd_r,
    x_s,
    x_r,
    f_s,
    f_r,
    h_s,
    h_r,
    o_s,
    o_r,
):
    z, c, y, x = (lax.axis_index(a) for a in EVERY)
    rows = nz * PAIR
    half = rows // 2
    kept = nz * SLOTS
    t = y * 4 + x

    def peer(da, db):
        py = lax.rem(y + (1 - c) * da + c * db, 4)
        px = lax.rem(x + c * da + (1 - c) * db, 4)
        return (z, c, py, px)

    def tid(da, db):
        _, _, py, px = peer(da, db)
        return py * 4 + px

    def other_tid(da, db):
        py = lax.rem(y + c * da + (1 - c) * db, 4)
        px = lax.rem(x + (1 - c) * da + c * db, 4)
        return py * 4 + px

    def at_z(dz):
        return (lax.rem(z + dz, nz), c, y, x)

    partner = (z, 1 - c, y, x)

    def rc(src, dst, ss, rs, dev):
        return pltpu.make_async_remote_copy(
            src_ref=src, dst_ref=dst, send_sem=ss, recv_sem=rs, device_id=dev, device_id_type=MESH
        )

    def at_other(dz):
        return (lax.rem(z + dz, nz), 1 - c, y, x)

    def w_rows(dz, core):
        return pl.ds(pl.multiple_of((lax.rem(z + dz, nz) * 2 + core) * 64, 64), 64)

    rate = rate_ref[0]
    down = nz - 1

    def ring(way, s):
        dz = (nz - s + 1) if way == 0 else (s - 1)
        ref = wfull.at[w_rows(dz, c)]
        return rc(ref, ref, wr_s.at[way, s], wr_r.at[way, s], at_z(1 if way == 0 else down))

    def ring_got(way, s):
        dz = nz - s if way == 0 else s
        ref = wfull.at[w_rows(dz, c)]
        return rc(ref, ref, wr_s.at[way, s], wr_r.at[way, s], at_z(1 if way == 0 else down))

    def pass_on(dz, core):
        ref = wfull.at[w_rows(dz, core)]
        return rc(ref, ref, wd_s.at[dz], wd_r.at[dz], partner)

    far = nz // 2

    def ring_step(s):
        ring_got(0, s).wait_recv()
        if s < far:
            ring(0, s + 1).start()
        pass_on(nz - s, c).start()
        if s < far:
            ring_got(1, s).wait_recv()
            if s < far - 1:
                ring(1, s + 1).start()
            pass_on(s, c).start()

    barrier = pltpu.get_barrier_semaphore()

    @pl.loop(1, nz)
    def _(dz):
        pl.semaphore_signal(barrier, inc=1, device_id=at_z(dz), device_id_type=MESH)

    @pl.loop(1, 16)
    def _(k):
        pl.semaphore_signal(
            barrier, inc=1, device_id=peer(k // 4, lax.rem(k, 4)), device_id_type=MESH
        )

    pl.semaphore_signal(barrier, inc=1, device_id=partner, device_id_type=MESH)

    cols = pl.ds(pl.multiple_of(t * LANES, LANES), LANES)
    local = [
        pltpu.make_async_copy(cot_hbm.at[:, cols], cot_s, loc.at[0]),
        pltpu.make_async_copy(stream_hbm.at[:, cols], str_s, loc.at[1]),
        pltpu.make_async_copy(gate_hbm, wcat.at[0, :, pl.ds(0, LANES)], loc.at[2]),
        pltpu.make_async_copy(up_hbm, wcat.at[0, :, pl.ds(LANES, LANES)], loc.at[3]),
        pltpu.make_async_copy(down_hbm, down_v, loc.at[4]),
        pltpu.make_async_copy(out_weight_hbm, wfull.at[w_rows(0, c)], loc.at[7]),
    ]
    for copy in local:
        copy.start()

    experts = iota((nz, LANES), 0)
    named = [(experts == routes_ref[k : k + 1, :]).astype(F32) for k in range(2)]
    before = (iota((LANES, LANES), 0) < iota((LANES, LANES), 1)).astype(BF)
    count = dot((named[0] + named[1]).astype(BF), before)
    rank = [
        jnp.sum(named[k] * count, axis=0, keepdims=True).astype(jnp.int32) for k in range(2)
    ]
    slot = [routes_ref[k : k + 1, :] * PAIR + rank[k] for k in range(2)]
    places = iota((rows, LANES), 0)
    acc[...] = jnp.zeros_like(acc)
    local[0].wait()
    local[1].wait()
    cot = cot_s[...].astype(F32)
    packed = dot(
        jnp.logical_or(places == slot[0] + SLOTS, places == slot[1] + SLOTS).astype(F32).astype(BF),
        str_s[...],
    )
    for k in range(2):
        scaled = (weights_ref[:, k : k + 1] * cot).astype(BF)
        packed = packed + dot((places == slot[k]).astype(F32).astype(BF), scaled)
    sbuf[...] = packed.astype(BF)

    pl.semaphore_wait(barrier, nz - 1 + 15 + 1)

    mine = pl.ds(pl.multiple_of(z * PAIR, 8), PAIR)
    for k in range(1, nz):
        dz = nz // 2 + (k // 2 if k % 2 == 0 else -(k // 2))
        there = pl.ds(pl.multiple_of(lax.rem(z + dz, nz) * PAIR, 8), PAIR)
        rc(sbuf.at[there], xs.at[c, t, mine], z_s.at[dz], z_r.at[dz], at_z(dz)).start()
    own = pltpu.make_async_copy(sbuf.at[mine], xs.at[c, t, mine], loc.at[5])
    own.start()
    steps = iota((LANES, 1), 0).astype(F32)
    scale = k_ref.shape[1] ** -0.5
    block_decay = jnp.exp(-rate * jnp.full((1, 512), float(LANES), F32))
    chip_decay = jnp.exp(-rate * jnp.full((1, 512), 2.0 * LANES, F32))
    keys = (k_ref[...].astype(F32) * scale).astype(BF)
    vals = v_ref[...]

    def split(a):
        high = a.astype(BF)
        return high, (a - high.astype(F32)).astype(BF)

    def dot2(a, b, left=1, right=0):
        high, low = split(a)
        return dot(high, b, left, right) + dot(low, b, left, right)

    def dot_2(a, b, left=1, right=0):
        high, low = split(b)
        return dot(a, high, left, right) + dot(a, low, left, right)

    leave = jnp.exp(-rate * (LANES - 1.0 - steps))
    state[c] = dot2(keys.astype(F32) * leave, vals, 0, 0)
    state_copy = rc(state.at[c], state.at[c], x_s.at[0], x_r.at[0], partner)
    state_copy.start()
    local[5].wait()
    ring(0, 1).start()
    ring(1, 1).start()
    pass_on(0, c).start()
    local[2].wait()
    local[3].wait()
    weight_copy = rc(wcat.at[0], wcat.at[1], w_s, w_r, partner)
    weight_copy.start()
    local[4].wait()
    own.wait()
    for dz in range(1, nz):
        here = pl.ds(pl.multiple_of(lax.rem(z + nz - dz, nz) * PAIR, 8), PAIR)
        rc(sbuf.at[mine], xs.at[c, t, here], z_s.at[dz], z_r.at[dz], at_z(dz)).wait_recv()

    def product(core, piece):
        a = xs[core, piece]
        deep = pl.ds(pl.multiple_of(piece * LANES, LANES), LANES)
        acc[core, :, 0:256] += dot(a, wcat[0, deep, :])
        acc[core, :, 256:384] += dot(a, down_v[:, deep], 1, 1)

    first = pl.ds(0, half)
    last = pl.ds(half, half)

    def a_copy(k, piece):
        part = (slice(None), slice(None), first, last)[k]
        ref = xs.at[c, piece] if k < 2 else xs.at[c, piece, part]
        return rc(ref, ref, a_s.at[k], a_r.at[k], peer(1 if k % 2 == 0 else 3, 0))

    def b_copy(i, k, piece):
        part = (slice(None), slice(None), first, last)[k]
        ref = xs.at[c, piece] if k < 2 else xs.at[c, piece, part]
        return rc(ref, ref, b_s.at[i, k], b_r.at[i, k], peer(0, 1 if k % 2 == 0 else 3))

    def d_copy(i, j, core, piece):
        ref = xs.at[core, piece]
        return rc(ref, ref, d_s.at[i, j], d_r.at[i, j], partner)

    def spread(i, piece):
        b_copy(i, 0, piece).start()
        b_copy(i, 1, piece).start()
        d_copy(i, 0, c, piece).start()

    a_copy(0, t).start()
    a_copy(1, t).start()
    spread(0, t)
    product(c, t)
    piece = tid(3, 0)
    a_copy(0, piece).wait_recv()
    a_copy(2, piece).start()
    spread(1, piece)
    other = tid(1, 0)
    a_copy(1, other).wait_recv()
    a_copy(3, other).start()
    spread(2, other)
    product(c, piece)
    product(c, other)
    piece = tid(2, 0)
    a_copy(2, piece).wait_recv()
    a_copy(3, piece).wait_recv()
    spread(3, piece)
    product(c, piece)

    rows_here = pl.ds(pl.multiple_of(c * 128, 128), 128)
    rows_there = pl.ds(pl.multiple_of((1 - c) * 128, 128), 128)

    def slice_of(dz):
        return pl.ds(pl.multiple_of(lax.rem(z + dz, nz) * 8, 8), 8)

    def exchange(src, dst, ss, rs):
        for k in range(1, nz):
            dz = nz // 2 + (k // 2 if k % 2 == 0 else -(k // 2))
            rc(src.at[slice_of(dz)], dst.at[slice_of(0)], ss.at[dz], rs.at[dz], at_z(dz)).start()
        mine_copy = pltpu.make_async_copy(src.at[slice_of(0)], dst.at[slice_of(0)], ss.at[0])
        mine_copy.start()

    def exchanged(src, dst, ss, rs):
        pltpu.make_async_copy(src.at[slice_of(0)], dst.at[slice_of(0)], ss.at[0]).wait()
        for dz in range(1, nz):
            rc(
                src.at[slice_of(0)], dst.at[slice_of(nz - dz)], ss.at[dz], rs.at[dz], at_z(dz)
            ).wait_recv()

    def exchange_sent(src, dst, ss, rs):
        for dz in range(1, nz):
            rc(src.at[slice_of(0)], dst.at[slice_of(0)], ss.at[dz], rs.at[dz], at_z(dz)).wait_send()

    rc(state.at[1 - c], state.at[1 - c], x_s.at[0], x_r.at[0], partner).wait_recv()
    half_state[...] = block_decay * state[0, rows_here, :] + state[1, rows_here, :]
    exchange(half_state, slices, f_s.at[0], f_r.at[0])

    def offset(i):
        return (lax.rem(i + 1, 3) + 1) * jnp.minimum(i, 1)

    @pl.loop(0, 4)
    def _(i):
        da = offset(i)
        left, right, far = tid(da, 3), tid(da, 1), tid(da, 2)
        b_copy(i, 0, left).wait_recv()
        b_copy(i, 2, left).start()
        d_copy(i, 1, c, left).start()
        b_copy(i, 1, right).wait_recv()
        b_copy(i, 3, right).start()
        d_copy(i, 2, c, right).start()
        product(c, left)
        product(c, right)
        b_copy(i, 2, far).wait_recv()
        b_copy(i, 3, far).wait_recv()
        d_copy(i, 3, c, far).start()
        product(c, far)
        for j in range(4):
            piece = other_tid(da, (0, 3, 1, 2)[j])
            d_copy(i, j, 1 - c, piece).wait_recv()
            product(1 - c, piece)
        for s in range(1, 5):
            @pl.when(i == s - 1)
            def _():
                ring_step(s)

    @pl.loop(0, 2 * rows // 80)
    def _(k):
        core = k // (rows // 80)
        at = pl.ds(pl.multiple_of(lax.rem(k, rows // 80) * 80, 8), 80)
        lane_row = iota((80, LANES), 0)
        is_in = jnp.logical_or(
            jnp.logical_and(lane_row >= 20, lane_row < 40), lane_row >= 60
        )
        pre_gate = acc[core, at, 0:128]
        pre_up = acc[core, at, 128:256]
        grad_hidden = pltpu.roll(acc[core, at, 256:384], 20, axis=0)
        gate = jax.nn.sigmoid(pre_gate)
        active = pre_gate * gate
        hidden = active * pre_up
        grad_gate = grad_hidden * pre_up * (gate * (1.0 + pre_gate * (1.0 - gate)))
        grad_up = grad_hidden * active
        wide[core, at, 0:128] = jnp.where(is_in, grad_gate, 0.0).astype(BF)
        wide[core, at, 128:256] = jnp.where(is_in, grad_up, 0.0).astype(BF)
        wide[core, at, 256:384] = jnp.where(is_in, 0.0, pltpu.roll(hidden, 60, axis=0)).astype(BF)

    exchanged(half_state, slices, f_s.at[0], f_r.at[0])
    running = jnp.zeros((8, 512), F32)
    for e in range(nz):
        scanned[e * 8 : e * 8 + 8, :] = running
        running = chip_decay * running + slices[e * 8 : e * 8 + 8, :]
    exchange(scanned, carried.at[rows_here], f_s.at[1], f_r.at[1])
    ring_step(5)

    low = iota((kept, rows), 0)
    pick = (iota((kept, rows), 1) == low + SLOTS * ((low * 3277) // 65536) + SLOTS)
    pick = pick.astype(F32).astype(BF)
    gsend[...] = dot(pick, wide[1 - c, :, 0:256]).astype(BF)
    grad_copy = rc(gsend, gpart, g_s, g_r, partner)
    grad_copy.start()
    gown[...] = dot(pick, wide[c, :, 0:256]).astype(BF)
    weight_copy.wait_recv()
    grad_copy.wait_recv()

    def partial_in(piece):
        deep = pl.ds(pl.multiple_of(piece * LANES, LANES), LANES)
        return dot(gown[...], wcat[0, deep, :], 1, 1) + dot(gpart[...], wcat[1, deep, :], 1, 1)

    def q_copy(da):
        return rc(pbuf.at[da - 1], qbuf.at[da - 1], q_s.at[da - 1], q_r.at[da - 1], peer(da, 0))

    for da in (2, 1, 3):

        @pl.loop(0, 4)
        def _(db):
            pbuf[da - 1, db] = partial_in(tid(da, db)).astype(BF)

        q_copy(da).start()

    @pl.loop(0, 4)
    def _(db):
        pown[db] = partial_in(tid(0, db))

    ring_step(6)

    for core in range(2):
        wide_t[core] = wide[core].T

    @pl.loop(0, 16)
    def _(piece):
        deep = pl.ds(pl.multiple_of(piece * LANES, LANES), LANES)
        total = dot(wide_t[0], xs[0, piece]) + dot(wide_t[1], xs[1, piece])
        gd_ref[:, deep] = total[256:384].astype(BF)
        gg_ref[deep, :] = total[0:128].T.astype(BF)
        gu_ref[deep, :] = total[128:256].T.astype(BF)

    ring_step(7)
    for da in (1, 3, 2):
        q_copy(da).wait_recv()

    def v_copy(db):
        return rc(tsum.at[db - 1], vbuf.at[db - 1], v_s.at[db - 1], v_r.at[db - 1], peer(0, db))

    for db in (2, 1, 3):
        whole = pown[db]
        for da in range(3):
            whole = whole + qbuf[da, db].astype(F32)
        tsum[db - 1] = whole.astype(BF)
        v_copy(db).start()
    whole = pown[0]
    for da in range(3):
        whole = whole + qbuf[da, 0].astype(F32)
    town[...] = whole
    exchanged(scanned, carried.at[rows_here], f_s.at[1], f_r.at[1])
    carry_copy = rc(carried.at[rows_here], carried.at[rows_here], x_s.at[1], x_r.at[1], partner)
    carry_copy.start()
    for db in (1, 3, 2):
        v_copy(db).wait_recv()
    whole = town[...]
    for db in range(3):
        whole = whole + vbuf[db].astype(F32)
    low = iota((nz * BACK, kept), 0)
    block = (low * 2731) // 65536
    spreadm = jnp.logical_and(
        iota((nz * BACK, kept), 1) == low - (BACK - SLOTS) * block, low - BACK * block < SLOTS
    )
    rsend[...] = dot(spreadm.astype(F32).astype(BF), whole.astype(BF)).astype(BF)

    here = pl.ds(pl.multiple_of(z * BACK, 8), BACK)
    for k in range(1, nz):
        dz = nz // 2 + (k // 2 if k % 2 == 0 else -(k // 2))
        there = pl.ds(pl.multiple_of(lax.rem(z + dz, nz) * BACK, 8), BACK)
        rc(rsend.at[there], ret.at[here], r_s.at[dz], r_r.at[dz], at_z(dz)).start()
    own = pltpu.make_async_copy(rsend.at[here], ret.at[here], loc.at[6])
    own.start()
    places = iota((nz * BACK, LANES), 0)
    take = jnp.logical_or(
        places == routes_ref[0:1, :] * BACK + rank[0], places == routes_ref[1:2, :] * BACK + rank[1]
    )
    take = take.astype(F32).astype(BF)
    own.wait()

    distance = iota((LANES, LANES), 0) - iota((LANES, LANES), 1)
    mask = jnp.where(
        distance >= 0, jnp.exp(-rate * jnp.maximum(distance, 0).astype(F32)), 0.0
    )
    enter = jnp.exp(-rate * (steps + 1.0))
    queries = q_ref[...]
    rc(carried.at[rows_there], carried.at[rows_there], x_s.at[1], x_r.at[1], partner).wait_recv()

    carry_copy.wait_send()

    @pl.when(c == 1)
    def _():
        carried[...] = block_decay * carried[...] + state[0]

    scores[...] = dot(queries, keys, 1, 1) * mask
    retained = dot2(scores[...], vals) + enter * dot_2(queries, carried[...])
    centered = retained - jnp.mean(retained, axis=-1, keepdims=True)
    inv = lax.rsqrt(jnp.mean(centered * centered, axis=-1, keepdims=True) + NORM_EPS)
    norm_s[...] = centered * inv
    inv_s[...] = inv
    mixes[c] = norm_s[...].astype(BF)
    mix_copy = rc(mixes.at[c], mixes.at[c], x_s.at[2], x_r.at[2], partner)
    mix_copy.start()
    ring_step(8)
    for dz in range(1, nz):
        there = pl.ds(pl.multiple_of(lax.rem(z + nz - dz, nz) * BACK, 8), BACK)
        rc(rsend.at[here], ret.at[there], r_s.at[dz], r_r.at[dz], at_z(dz)).wait_recv()
    mids[c, :, cols] = (cot_s[...].astype(F32) + dot(take, ret[...], 0, 0)).astype(BF)

    @pl.loop(1, 16)
    def _(k):
        dev = peer(k // 4, lax.rem(k, 4))
        rc(mids.at[c, :, cols], mids.at[c, :, cols], m_s.at[k], m_r.at[k], dev).start()

    @pl.loop(1, 16)
    def _(k):
        back = tid(lax.rem(4 - k // 4, 4), lax.rem(4 - lax.rem(k, 4), 4))
        theirs = pl.ds(pl.multiple_of(back * LANES, LANES), LANES)
        dev = peer(k // 4, lax.rem(k, 4))
        rc(mids.at[c, :, cols], mids.at[c, :, theirs], m_s.at[k], m_r.at[k], dev).wait_recv()

    mid_copy = rc(mids.at[c], mids.at[c], x_s.at[3], x_r.at[3], partner)
    mid_copy.start()
    for dz in range(nz):
        pass_on(dz, 1 - c).wait_recv()
    head_grad = dot(mids[c], wfull[...])
    normed = norm_s[...]
    grad_ret = inv_s[...] * (
        head_grad
        - jnp.mean(head_grad, axis=-1, keepdims=True)
        - normed * jnp.mean(head_grad * normed, axis=-1, keepdims=True)
    )
    start = jnp.exp(-rate * steps)
    back_state[c] = dot_2(
        queries, start * grad_ret, 0, 0
    )
    back_copy = rc(back_state.at[c], back_state.at[c], x_s.at[4], x_r.at[4], partner)
    back_copy.start()

    rc(mixes.at[1 - c], mixes.at[1 - c], x_s.at[2], x_r.at[2], partner).wait_recv()
    rc(mids.at[1 - c], mids.at[1 - c], x_s.at[3], x_r.at[3], partner).wait_recv()

    def partial_out(way, dz):
        wide_cols = pl.ds(pl.multiple_of(lax.rem(z + dz, nz) * LANES, LANES), LANES)
        prods[way] = dot(mids[0, :, wide_cols], mixes[0], 0, 0) + dot(
            mids[1, :, wide_cols], mixes[1], 0, 0
        )
        return prods[way, pl.ds(pl.multiple_of(c * 64, 64), 64), :]

    def up_copy(s):
        return rc(up_s.at[s], up_r.at[s], o_s.at[0, s], o_r.at[0, s], at_z(1))

    def dn_copy(s):
        return rc(dn_s.at[s], dn_r.at[s], o_s.at[1, s], o_r.at[1, s], at_z(down))

    def sum_step(s):
        up = partial_out(0, far - s)
        if s > 0:
            up_copy(s - 1).wait_recv()
            up = up + up_r[s - 1].astype(F32)
        up_s[s] = up.astype(BF)
        up_copy(s).start()
        if s < far - 1:
            dn = partial_out(1, nz - (far - 1 - s))
            if s > 0:
                dn_copy(s - 1).wait_recv()
                dn = dn + dn_r[s - 1].astype(F32)
            dn_s[s] = dn.astype(BF)
            dn_copy(s).start()

    sum_step(0)
    rc(back_state.at[1 - c], back_state.at[1 - c], x_s.at[4], x_r.at[4], partner).wait_recv()
    half_back[...] = (back_state[0, rows_here, :] + block_decay * back_state[1, rows_here, :]).astype(BF)
    exchange(half_back, bslices, h_s.at[0], h_r.at[0])
    sum_step(1)
    score_grad = dot2(grad_ret, vals, 1, 1) * mask
    grad_q = dot2(score_grad, keys)
    high, low = split(grad_ret)
    c_high, c_low = split(carried[...])
    grad_q = grad_q + enter * (dot(high, c_high, 1, 1) + dot(low, c_high, 1, 1) + dot(high, c_low, 1, 1))
    gq_ref[...] = grad_q.astype(BF)
    sum_step(2)
    exchanged(half_back, bslices, h_s.at[0], h_r.at[0])
    running = jnp.zeros((8, 512), F32)
    for e in range(nz - 1, -1, -1):
        bscanned[e * 8 : e * 8 + 8, :] = running.astype(BF)
        running = chip_decay * running + bslices[e * 8 : e * 8 + 8, :].astype(F32)
    exchange(bscanned, future.at[rows_here], h_s.at[1], h_r.at[1])
    sum_step(3)
    score_t = scores[...]
    s_high, s_low = split(score_t)
    grad_v = dot(s_high, high, 0, 0) + dot(s_low, high, 0, 0) + dot(s_high, low, 0, 0)
    grad_k = dot2(score_grad, queries, 0, 0)
    sum_step(4)
    exchanged(bscanned, future.at[rows_here], h_s.at[1], h_r.at[1])
    future_copy = rc(future.at[rows_here], future.at[rows_here], x_s.at[5], x_r.at[5], partner)
    future_copy.start()
    sum_step(5)
    rc(future.at[rows_there], future.at[rows_there], x_s.at[5], x_r.at[5], partner).wait_recv()
    trail = jnp.exp(-rate * (LANES - steps))
    ahead = future[...].astype(F32)
    ahead = jnp.where(c == 0, back_state[1] + block_decay * ahead, ahead)
    gv_ref[...] = (grad_v + trail * dot_2(keys, ahead)).astype(BF)
    gk_ref[...] = ((grad_k + trail * dot_2(vals, ahead, 1, 1)) * scale).astype(BF)
    sum_step(6)
    sum_step(7)
    total = partial_out(0, 0)
    dn_copy(far - 2).wait_recv()
    total = total + dn_r[far - 2].astype(F32)
    up_copy(far - 1).wait_recv()
    gow_ref[...] = total + up_r[far - 1].astype(F32)

    for s in range(far):
        up_copy(s).wait_send()
        ring(0, s + 1).wait_send()
        if s < far - 1:
            dn_copy(s).wait_send()
            ring(1, s + 1).wait_send()
    for dz in range(nz):
        pass_on(dz, c).wait_send()
    exchange_sent(half_state, slices, f_s.at[0], f_r.at[0])
    exchange_sent(scanned, carried.at[rows_here], f_s.at[1], f_r.at[1])
    exchange_sent(half_back, bslices, h_s.at[0], h_r.at[0])
    exchange_sent(bscanned, future.at[rows_here], h_s.at[1], h_r.at[1])
    for copy in (state_copy, mix_copy, mid_copy, back_copy, future_copy):
        copy.wait_send()
    for dz in range(1, nz):
        rc(sbuf.at[mine], xs.at[c, t, mine], z_s.at[dz], z_r.at[dz], at_z(dz)).wait_send()
        rc(rsend.at[here], ret.at[here], r_s.at[dz], r_r.at[dz], at_z(dz)).wait_send()
    weight_copy.wait_send()
    grad_copy.wait_send()
    for k in range(4):
        a_copy(k, t).wait_send()

    @pl.loop(0, 4)
    def _(i):
        for k in range(4):
            b_copy(i, k, t).wait_send()
            d_copy(i, k, c, t).wait_send()

    for k in range(1, 4):
        q_copy(k).wait_send()
        v_copy(k).wait_send()

    @pl.loop(1, 16)
    def _(k):
        dev = peer(k // 4, lax.rem(k, 4))
        rc(mids.at[c, :, cols], mids.at[c, :, cols], m_s.at[k], m_r.at[k], dev).wait_send()


def local(
    cotangent,
    stream,
    routes,
    route_weights,
    gate_proj,
    up_proj,
    down_proj,
    out_weight,
    queries,
    keys,
    values,
    decay_rate,
):
    nz = lax.axis_size("z")
    width = cotangent.shape[1]
    rows, kept = nz * PAIR, nz * SLOTS
    far = nz // 2
    any_ = pl.BlockSpec(memory_space=pl.ANY)
    vmem = pl.BlockSpec(memory_space=pltpu.VMEM)
    dma = pltpu.SemaphoreType.DMA
    grads = pl.pallas_call(
        functools.partial(kernel, nz),
        out_shape=(
            jax.ShapeDtypeStruct((width, LANES), BF),
            jax.ShapeDtypeStruct((width, LANES), BF),
            jax.ShapeDtypeStruct((LANES, width), BF),
            jax.ShapeDtypeStruct(out_weight.shape, F32),
            jax.ShapeDtypeStruct(queries.shape, BF),
            jax.ShapeDtypeStruct(keys.shape, BF),
            jax.ShapeDtypeStruct(values.shape, BF),
        ),
        in_specs=[vmem, vmem]
        + [any_] * 6
        + [vmem, vmem, vmem, pl.BlockSpec(memory_space=pltpu.SMEM)],
        out_specs=(vmem,) * 7,
        scratch_shapes=[
            pltpu.VMEM((2, width, 2 * LANES), BF),
            pltpu.VMEM((LANES, width), BF),
            pltpu.VMEM((LANES, LANES), BF),
            pltpu.VMEM((LANES, LANES), BF),
            pltpu.VMEM((rows, LANES), BF),
            pltpu.VMEM((2, 16, rows, LANES), BF),
            pltpu.VMEM((2, rows, 3 * LANES), F32),
            pltpu.VMEM((2, rows, 3 * LANES), BF),
            pltpu.VMEM((2, 3 * LANES, rows), BF),
            pltpu.VMEM((kept, 2 * LANES), BF),
            pltpu.VMEM((kept, 2 * LANES), BF),
            pltpu.VMEM((kept, 2 * LANES), BF),
            pltpu.VMEM((3, 4, kept, LANES), BF),
            pltpu.VMEM((4, kept, LANES), F32),
            pltpu.VMEM((3, 4, kept, LANES), BF),
            pltpu.VMEM((3, kept, LANES), BF),
            pltpu.VMEM((kept, LANES), F32),
            pltpu.VMEM((3, kept, LANES), BF),
            pltpu.VMEM((nz * BACK, LANES), BF),
            pltpu.VMEM((nz * BACK, LANES), BF),
            pltpu.VMEM((2, LANES, width), BF),
            pltpu.VMEM((width, 512), BF),
            pltpu.VMEM((2, 256, 512), F32),
            pltpu.VMEM((128, 512), F32),
            pltpu.VMEM((128, 512), F32),
            pltpu.VMEM((128, 512), F32),
            pltpu.VMEM((256, 512), F32),
            pltpu.VMEM((2, LANES, 512), BF),
            pltpu.VMEM((LANES, LANES), F32),
            pltpu.VMEM((LANES, 512), F32),
            pltpu.VMEM((LANES, 1), F32),
            pltpu.VMEM((2, 256, 512), F32),
            pltpu.VMEM((128, 512), BF),
            pltpu.VMEM((128, 512), BF),
            pltpu.VMEM((128, 512), BF),
            pltpu.VMEM((256, 512), BF),
            pltpu.VMEM((2, LANES, 512), F32),
            pltpu.VMEM((far, 64, 512), BF),
            pltpu.VMEM((far, 64, 512), BF),
            pltpu.VMEM((far - 1, 64, 512), BF),
            pltpu.VMEM((far - 1, 64, 512), BF),
            dma((8,)),
            dma((nz,)),
            dma((nz,)),
            dma,
            dma,
            dma((4,)),
            dma((4,)),
            dma((4, 4)),
            dma((4, 4)),
            dma((4, 4)),
            dma((4, 4)),
            dma,
            dma,
            dma((3,)),
            dma((3,)),
            dma((3,)),
            dma((3,)),
            dma((nz,)),
            dma((nz,)),
            dma((16,)),
            dma((16,)),
            dma((2, far + 1)),
            dma((2, far + 1)),
            dma((nz,)),
            dma((nz,)),
            dma((6,)),
            dma((6,)),
            dma((2, nz)),
            dma((2, nz)),
            dma((2, nz)),
            dma((2, nz)),
            dma((2, far)),
            dma((2, far)),
        ],
        compiler_params=pltpu.CompilerParams(
            collective_id=0, has_side_effects=True, vmem_limit_bytes=58 * 2**20
        ),
        name="layer_backward",
    )(
        routes.T,
        route_weights,
        cotangent,
        stream,
        gate_proj[0],
        up_proj[0],
        down_proj[0],
        out_weight,
        queries,
        keys,
        values,
        decay_rate,
    )
    return tuple(g[None] for g in grads[:3]) + tuple(grads[3:])


def solution(mesh):
    blocks, heads = mesh.devices.shape
    split = Mesh(mesh.devices.reshape(blocks // 2, 2, 4, heads // 4), EVERY)
    tokens = P(SP, None)
    tiles = P(SP, TP)
    in_specs = (
        tokens,
        tokens,
        tokens,
        tokens,
        P(SP, None, TP),
        P(SP, None, TP),
        P(SP, TP, None),
        tiles,
        tiles,
        tiles,
        tiles,
        P(TP),
    )
    out_specs = (
        P(SP, None, TP),
        P(SP, None, TP),
        P(SP, TP, None),
        tiles,
        tiles,
        tiles,
        tiles,
    )
    return jax.shard_map(local, mesh=split, in_specs=in_specs, out_specs=out_specs, check_vma=False)
```

```python
import functools

import jax
import jax.numpy as jnp
from jax import lax
from jax.experimental import pallas as pl
from jax.experimental.pallas import tpu as pltpu
from jax.sharding import Mesh
from jax.sharding import PartitionSpec as P

SP = ("z", "c")
TP = ("y", "x")
EVERY = ("z", "c", "y", "x")
NORM_EPS = 1.0
SLOTS = 20
PAIR = 2 * SLOTS
BACK = 24
LANES = 128
BF = jnp.bfloat16
F32 = jnp.float32
MESH = pl.DeviceIdType.MESH


def dot(a, b, left=1, right=0):
    return lax.dot_general(a, b, (((left,), (right,)), ((), ())), preferred_element_type=F32)


def iota(shape, dim):
    return lax.broadcasted_iota(jnp.int32, shape, dim)


def kernel(
    nz,
    routes_ref,
    weights_ref,
    cot_hbm,
    stream_hbm,
    gate_hbm,
    up_hbm,
    down_hbm,
    out_weight_hbm,
    q_ref,
    k_ref,
    v_ref,
    rate_ref,
    gg_ref,
    gu_ref,
    gd_ref,
    gow_ref,
    gq_ref,
    gk_ref,
    gv_ref,
    wcat,
    down_v,
    cot_s,
    str_s,
    sbuf,
    xs,
    acc,
    wide,
    wide_t,
    gsend,
    gown,
    gpart,
    pbuf,
    pown,
    qbuf,
    tsum,
    town,
    vbuf,
    rsend,
    ret,
    mids,
    wfull,
    state,
    half_state,
    slices,
    scanned,
    carried,
    mixes,
    scores,
    norm_s,
    inv_s,
    back_state,
    whole_back,
    bslices,
    bscanned,
    future,
    up_s,
    up_r,
    dn_s,
    dn_r,
    part_v,
    part_k,
    ret_s,
    sgrad,
    gow_s,
    entered,
    loc,
    z_s,
    z_r,
    w_s,
    w_r,
    a_s,
    a_r,
    b_s,
    b_r,
    d_s,
    d_r,
    g_s,
    g_r,
    q_s,
    q_r,
    v_s,
    v_r,
    r_s,
    r_r,
    m_s,
    m_r,
    wr_s,
    wr_r,
    wd_s,
    wd_r,
    x_s,
    x_r,
    f_s,
    f_r,
    h_s,
    h_r,
    o_s,
    o_r,
):
    z, c, y, x = (lax.axis_index(a) for a in EVERY)
    rows = nz * PAIR
    half = rows // 2
    kept = nz * SLOTS
    t = y * 4 + x

    def peer(da, db):
        py = lax.rem(y + (1 - c) * da + c * db, 4)
        px = lax.rem(x + c * da + (1 - c) * db, 4)
        return (z, c, py, px)

    def tid(da, db):
        _, _, py, px = peer(da, db)
        return py * 4 + px

    def other_tid(da, db):
        py = lax.rem(y + c * da + (1 - c) * db, 4)
        px = lax.rem(x + (1 - c) * da + c * db, 4)
        return py * 4 + px

    def at_z(dz):
        return (lax.rem(z + dz, nz), c, y, x)

    partner = (z, 1 - c, y, x)

    def rc(src, dst, ss, rs, dev):
        return pltpu.make_async_remote_copy(
            src_ref=src, dst_ref=dst, send_sem=ss, recv_sem=rs, device_id=dev, device_id_type=MESH
        )

    def at_other(dz):
        return (lax.rem(z + dz, nz), 1 - c, y, x)

    def w_rows(dz, core):
        return pl.ds(pl.multiple_of((lax.rem(z + dz, nz) * 2 + core) * 64, 64), 64)

    rate = rate_ref[0]
    down = nz - 1

    def ring(way, s):
        dz = (nz - s + 1) if way == 0 else (s - 1)
        ref = wfull.at[w_rows(dz, c)]
        return rc(ref, ref, wr_s.at[way, s], wr_r.at[way, s], at_z(1 if way == 0 else down))

    def ring_got(way, s):
        dz = nz - s if way == 0 else s
        ref = wfull.at[w_rows(dz, c)]
        return rc(ref, ref, wr_s.at[way, s], wr_r.at[way, s], at_z(1 if way == 0 else down))

    def pass_on(dz, core):
        ref = wfull.at[w_rows(dz, core)]
        return rc(ref, ref, wd_s.at[dz], wd_r.at[dz], partner)

    far = nz // 2

    def ring_step(s):
        ring_got(0, s).wait_recv()
        if s < far:
            ring(0, s + 1).start()
        pass_on(nz - s, c).start()
        if s < far:
            ring_got(1, s).wait_recv()
            if s < far - 1:
                ring(1, s + 1).start()
            pass_on(s, c).start()

    barrier = pltpu.get_barrier_semaphore()

    @pl.loop(1, nz)
    def _(dz):
        pl.semaphore_signal(barrier, inc=1, device_id=at_z(dz), device_id_type=MESH)

    @pl.loop(1, 16)
    def _(k):
        pl.semaphore_signal(
            barrier, inc=1, device_id=peer(k // 4, lax.rem(k, 4)), device_id_type=MESH
        )

    pl.semaphore_signal(barrier, inc=1, device_id=partner, device_id_type=MESH)

    cols = pl.ds(pl.multiple_of(t * LANES, LANES), LANES)
    local = [
        pltpu.make_async_copy(cot_hbm.at[:, cols], cot_s, loc.at[0]),
        pltpu.make_async_copy(stream_hbm.at[:, cols], str_s, loc.at[1]),
        pltpu.make_async_copy(gate_hbm, wcat.at[0, :, pl.ds(0, LANES)], loc.at[2]),
        pltpu.make_async_copy(up_hbm, wcat.at[0, :, pl.ds(LANES, LANES)], loc.at[3]),
        pltpu.make_async_copy(down_hbm, down_v, loc.at[4]),
        pltpu.make_async_copy(out_weight_hbm, wfull.at[w_rows(0, c)], loc.at[7]),
    ]
    for copy in local:
        copy.start()

    experts = iota((nz, LANES), 0)
    named = [(experts == routes_ref[k : k + 1, :]).astype(F32) for k in range(2)]
    before = (iota((LANES, LANES), 0) < iota((LANES, LANES), 1)).astype(BF)
    count = dot((named[0] + named[1]).astype(BF), before)
    rank = [
        jnp.sum(named[k] * count, axis=0, keepdims=True).astype(jnp.int32) for k in range(2)
    ]
    slot = [routes_ref[k : k + 1, :] * PAIR + rank[k] for k in range(2)]
    places = iota((rows, LANES), 0)
    acc[...] = jnp.zeros_like(acc)
    local[0].wait()
    local[1].wait()
    cot = cot_s[...].astype(F32)
    packed = dot(
        jnp.logical_or(places == slot[0] + SLOTS, places == slot[1] + SLOTS).astype(F32).astype(BF),
        str_s[...],
    )
    for k in range(2):
        scaled = (weights_ref[:, k : k + 1] * cot).astype(BF)
        packed = packed + dot((places == slot[k]).astype(F32).astype(BF), scaled)
    sbuf[...] = packed.astype(BF)

    pl.semaphore_wait(barrier, nz - 1 + 15 + 1)

    mine = pl.ds(pl.multiple_of(z * PAIR, 8), PAIR)
    for k in range(1, nz):
        dz = nz // 2 + (k // 2 if k % 2 == 0 else -(k // 2))
        there = pl.ds(pl.multiple_of(lax.rem(z + dz, nz) * PAIR, 8), PAIR)
        rc(sbuf.at[there], xs.at[c, t, mine], z_s.at[dz], z_r.at[dz], at_z(dz)).start()
    own = pltpu.make_async_copy(sbuf.at[mine], xs.at[c, t, mine], loc.at[5])
    own.start()
    steps = iota((LANES, 1), 0).astype(F32)
    scale = k_ref.shape[1] ** -0.5
    block_decay = jnp.exp(-rate * jnp.full((1, 512), float(LANES), F32))
    chip_decay = jnp.exp(-rate * jnp.full((1, 512), 2.0 * LANES, F32))
    keys = (k_ref[...].astype(F32) * scale).astype(BF)
    vals = v_ref[...]

    def split(a):
        high = a.astype(BF)
        return high, (a - high.astype(F32)).astype(BF)

    def dot2(a, b, left=1, right=0):
        high, low = split(a)
        return dot(high, b, left, right) + dot(low, b, left, right)

    def dot_2(a, b, left=1, right=0):
        high, low = split(b)
        return dot(a, high, left, right) + dot(a, low, left, right)

    leave = jnp.exp(-rate * (LANES - 1.0 - steps))
    state[c] = dot2(keys.astype(F32) * leave, vals, 0, 0)
    state_copy = rc(state.at[c], state.at[c], x_s.at[0], x_r.at[0], partner)
    state_copy.start()
    local[5].wait()
    ring(0, 1).start()
    ring(1, 1).start()
    pass_on(0, c).start()
    local[2].wait()
    local[3].wait()
    weight_copy = rc(wcat.at[0], wcat.at[1], w_s, w_r, partner)
    weight_copy.start()
    local[4].wait()
    own.wait()
    for dz in range(1, nz):
        here = pl.ds(pl.multiple_of(lax.rem(z + nz - dz, nz) * PAIR, 8), PAIR)
        rc(sbuf.at[mine], xs.at[c, t, here], z_s.at[dz], z_r.at[dz], at_z(dz)).wait_recv()

    def product(core, pieces):
        deep = [pl.ds(pl.multiple_of(piece * LANES, LANES), LANES) for piece in pieces]
        a = jnp.concatenate([xs[core, piece] for piece in pieces], axis=1)
        acc[core, :, 0:256] += dot(a, jnp.concatenate([wcat[0, d, :] for d in deep], axis=0))
        acc[core, :, 256:384] += dot(a, jnp.concatenate([down_v[:, d] for d in deep], axis=1), 1, 1)

    first = pl.ds(0, half)
    last = pl.ds(half, half)

    def a_copy(da):
        ref = xs.at[c, t]
        return rc(ref, ref, a_s.at[da], a_r.at[da], peer(da, 0))

    def a_got(da):
        ref = xs.at[c, tid(4 - da, 0)]
        rc(ref, ref, a_s.at[da], a_r.at[da], peer(da, 0)).wait_recv()

    def b_copy(i, k, piece):
        part = (slice(None), slice(None), first, last)[k]
        ref = xs.at[c, piece] if k < 2 else xs.at[c, piece, part]
        return rc(ref, ref, b_s.at[i, k], b_r.at[i, k], peer(0, 1 if k % 2 == 0 else 3))

    def d_copy(i, j, core, piece):
        ref = xs.at[core, piece]
        return rc(ref, ref, d_s.at[i, j], d_r.at[i, j], partner)

    def spread(i, piece):
        b_copy(i, 0, piece).start()
        b_copy(i, 1, piece).start()
        d_copy(i, 0, c, piece).start()

    for da in (1, 3, 2):
        a_copy(da).start()
    spread(0, t)
    ring_step(1)
    for i, da in ((1, 1), (2, 3), (3, 2)):
        a_got(da)
        spread(i, tid(4 - da, 0))
    ring_step(2)

    rows_here = pl.ds(pl.multiple_of(c * 128, 128), 128)
    rows_there = pl.ds(pl.multiple_of((1 - c) * 128, 128), 128)

    def slice_of(dz, n):
        return pl.ds(pl.multiple_of(lax.rem(z + dz, nz) * n, 8), n)

    def exchange(src, dst, ss, rs, n=8):
        for k in range(1, nz):
            dz = nz // 2 + (k // 2 if k % 2 == 0 else -(k // 2))
            rc(src.at[slice_of(dz, n)], dst.at[slice_of(0, n)], ss.at[dz], rs.at[dz], at_z(dz)).start()
        mine_copy = pltpu.make_async_copy(src.at[slice_of(0, n)], dst.at[slice_of(0, n)], ss.at[0])
        mine_copy.start()

    def exchanged(src, dst, ss, rs, n=8):
        pltpu.make_async_copy(src.at[slice_of(0, n)], dst.at[slice_of(0, n)], ss.at[0]).wait()
        for dz in range(1, nz):
            rc(
                src.at[slice_of(0, n)], dst.at[slice_of(nz - dz, n)], ss.at[dz], rs.at[dz], at_z(dz)
            ).wait_recv()

    def exchange_sent(src, dst, ss, rs, n=8):
        for dz in range(1, nz):
            rc(src.at[slice_of(0, n)], dst.at[slice_of(0, n)], ss.at[dz], rs.at[dz], at_z(dz)).wait_send()

    rc(state.at[1 - c], state.at[1 - c], x_s.at[0], x_r.at[0], partner).wait_recv()
    half_state[...] = block_decay * state[0, rows_here, :] + state[1, rows_here, :]

    def offset(i):
        return (lax.rem(i + 1, 3) + 1) * jnp.minimum(i, 1)

    def theirs_in(i):
        da = offset(i)
        pieces = [other_tid(da, db) for db in (0, 3, 1, 2)]
        for j in range(4):
            d_copy(i, j, 1 - c, pieces[j]).wait_recv()
        product(1 - c, pieces)

    @pl.loop(0, 4)
    def _(i):
        da = offset(i)
        left, right, far_piece = tid(da, 3), tid(da, 1), tid(da, 2)
        b_copy(i, 0, left).wait_recv()
        b_copy(i, 2, left).start()
        d_copy(i, 1, c, left).start()
        b_copy(i, 1, right).wait_recv()
        b_copy(i, 3, right).start()
        d_copy(i, 2, c, right).start()

        @pl.when(i > 0)
        def _():
            theirs_in(i - 1)

        b_copy(i, 2, far_piece).wait_recv()
        b_copy(i, 3, far_piece).wait_recv()
        d_copy(i, 3, c, far_piece).start()
        product(c, [tid(da, 0), left, right, far_piece])

        for s in range(3):

            @pl.when(i == s)
            def _():
                ring_step(3 + s)

    theirs_in(3)
    ring_step(6)
    exchange(half_state, slices, f_s.at[0], f_r.at[0])

    @pl.loop(0, 2 * rows // 80)
    def _(k):
        core = k // (rows // 80)
        at = pl.ds(pl.multiple_of(lax.rem(k, rows // 80) * 80, 8), 80)
        lane_row = iota((80, LANES), 0)
        is_in = jnp.logical_or(
            jnp.logical_and(lane_row >= 20, lane_row < 40), lane_row >= 60
        )
        pre_gate = acc[core, at, 0:128]
        pre_up = acc[core, at, 128:256]
        grad_hidden = pltpu.roll(acc[core, at, 256:384], 20, axis=0)
        gate = jax.nn.sigmoid(pre_gate)
        active = pre_gate * gate
        hidden = active * pre_up
        grad_gate = grad_hidden * pre_up * (gate * (1.0 + pre_gate * (1.0 - gate)))
        grad_up = grad_hidden * active
        wide[core, at, 0:128] = jnp.where(is_in, grad_gate, 0.0).astype(BF)
        wide[core, at, 128:256] = jnp.where(is_in, grad_up, 0.0).astype(BF)
        wide[core, at, 256:384] = jnp.where(is_in, 0.0, pltpu.roll(hidden, 60, axis=0)).astype(BF)

    low = iota((kept, rows), 0)
    pick = (iota((kept, rows), 1) == low + SLOTS * ((low * 3277) // 65536) + SLOTS)
    pick = pick.astype(F32).astype(BF)
    gsend[...] = dot(pick, wide[1 - c, :, 0:256]).astype(BF)
    grad_copy = rc(gsend, gpart, g_s, g_r, partner)
    grad_copy.start()
    gown[...] = dot(pick, wide[c, :, 0:256]).astype(BF)
    weight_copy.wait_recv()
    grad_copy.wait_recv()

    def partial_in(pieces):
        deep = [pl.ds(pl.multiple_of(piece * LANES, LANES), LANES) for piece in pieces]
        own_w, their_w = (jnp.concatenate([wcat[k, d, :] for d in deep], axis=0) for k in range(2))
        return dot(gown[...], own_w, 1, 1) + dot(gpart[...], their_w, 1, 1)

    def q_copy(da):
        return rc(pbuf.at[da - 1], qbuf.at[da - 1], q_s.at[da - 1], q_r.at[da - 1], peer(da, 0))

    for da in (2, 1, 3):

        for db in (0, 2):
            both = partial_in((tid(da, db), tid(da, db + 1))).astype(BF)
            pbuf[da - 1, db] = both[:, 0:LANES]
            pbuf[da - 1, db + 1] = both[:, LANES:]

        q_copy(da).start()

    for db in (0, 2):
        both = partial_in((tid(0, db), tid(0, db + 1)))
        pown[db] = both[:, 0:LANES]
        pown[db + 1] = both[:, LANES:]

    for core in range(2):
        wide_t[core] = wide[core].T

    def weight_grads(pair):
        deep = pl.ds(pl.multiple_of(pair * 2 * LANES, 2 * LANES), 2 * LANES)
        total = 0.0
        for core in range(2):
            both = jnp.concatenate([xs[core, pair * 2], xs[core, pair * 2 + 1]], axis=1)
            total = total + dot(wide_t[core], both)
        gd_ref[:, deep] = total[256:384].astype(BF)
        gg_ref[deep, :] = total[0:128].T.astype(BF)
        gu_ref[deep, :] = total[128:256].T.astype(BF)

    @pl.loop(0, 4)
    def _(pair):
        weight_grads(pair)

    @pl.loop(4, 8)
    def _(pair):
        weight_grads(pair)

    exchanged(half_state, slices, f_s.at[0], f_r.at[0])
    running = jnp.zeros((8, 512), F32)
    for e in range(nz):
        scanned[e * 8 : e * 8 + 8, :] = running.astype(BF)
        running = chip_decay * running + slices[e * 8 : e * 8 + 8, :]
    exchange(scanned, entered.at[rows_here], f_s.at[1], f_r.at[1])
    ring_step(7)
    for da in (1, 3, 2):
        q_copy(da).wait_recv()

    def v_copy(db):
        return rc(tsum.at[db - 1], vbuf.at[db - 1], v_s.at[db - 1], v_r.at[db - 1], peer(0, db))

    for db in (2, 1, 3):
        whole = pown[db]
        for da in range(3):
            whole = whole + qbuf[da, db].astype(F32)
        tsum[db - 1] = whole.astype(BF)
        v_copy(db).start()
    whole = pown[0]
    for da in range(3):
        whole = whole + qbuf[da, 0].astype(F32)
    town[...] = whole
    for db in (1, 3, 2):
        v_copy(db).wait_recv()
    whole = town[...]
    for db in range(3):
        whole = whole + vbuf[db].astype(F32)
    low = iota((nz * BACK, kept), 0)
    block = (low * 2731) // 65536
    spreadm = jnp.logical_and(
        iota((nz * BACK, kept), 1) == low - (BACK - SLOTS) * block, low - BACK * block < SLOTS
    )
    rsend[...] = dot(spreadm.astype(F32).astype(BF), whole.astype(BF)).astype(BF)

    here = pl.ds(pl.multiple_of(z * BACK, 8), BACK)
    for k in range(1, nz):
        dz = nz // 2 + (k // 2 if k % 2 == 0 else -(k // 2))
        there = pl.ds(pl.multiple_of(lax.rem(z + dz, nz) * BACK, 8), BACK)
        rc(rsend.at[there], ret.at[here], r_s.at[dz], r_r.at[dz], at_z(dz)).start()
    own = pltpu.make_async_copy(rsend.at[here], ret.at[here], loc.at[6])
    own.start()
    places = iota((nz * BACK, LANES), 0)
    take = jnp.logical_or(
        places == routes_ref[0:1, :] * BACK + rank[0], places == routes_ref[1:2, :] * BACK + rank[1]
    )
    take = take.astype(F32).astype(BF)
    own.wait()
    exchanged(scanned, entered.at[rows_here], f_s.at[1], f_r.at[1])
    carry_copy = rc(entered.at[rows_here], entered.at[rows_here], x_s.at[1], x_r.at[1], partner)
    carry_copy.start()

    distance = iota((LANES, LANES), 0) - iota((LANES, LANES), 1)
    mask = jnp.where(
        distance >= 0, jnp.exp(-rate * jnp.maximum(distance, 0).astype(F32)), 0.0
    )
    enter = jnp.exp(-rate * (steps + 1.0))
    queries = q_ref[...]
    rc(entered.at[rows_there], entered.at[rows_there], x_s.at[1], x_r.at[1], partner).wait_recv()

    inside = entered[...].astype(F32)
    carried[...] = jnp.where(c == 1, block_decay * inside + state[0], inside)
    scores[...] = dot(queries, keys, 1, 1) * mask
    retained = dot2(scores[...], vals) + enter * dot_2(queries, carried[...])
    centered = retained - jnp.mean(retained, axis=-1, keepdims=True)
    inv = lax.rsqrt(jnp.mean(centered * centered, axis=-1, keepdims=True) + NORM_EPS)
    norm_s[...] = centered * inv
    inv_s[...] = inv
    mixes[c] = norm_s[...].astype(BF)
    mix_copy = rc(mixes.at[c], mixes.at[c], x_s.at[2], x_r.at[2], partner)

    @pl.when(c == 0)
    def _():
        mix_copy.start()

    ring_step(8)
    for dz in range(1, nz):
        there = pl.ds(pl.multiple_of(lax.rem(z + nz - dz, nz) * BACK, 8), BACK)
        rc(rsend.at[here], ret.at[there], r_s.at[dz], r_r.at[dz], at_z(dz)).wait_recv()
    mids[c, :, cols] = (cot_s[...].astype(F32) + dot(take, ret[...], 0, 0)).astype(BF)

    @pl.loop(1, 16)
    def _(k):
        dev = peer(k // 4, lax.rem(k, 4))
        rc(mids.at[c, :, cols], mids.at[c, :, cols], m_s.at[k], m_r.at[k], dev).start()

    @pl.loop(1, 16)
    def _(k):
        back = tid(lax.rem(4 - k // 4, 4), lax.rem(4 - lax.rem(k, 4), 4))
        theirs = pl.ds(pl.multiple_of(back * LANES, LANES), LANES)
        dev = peer(k // 4, lax.rem(k, 4))
        rc(mids.at[c, :, cols], mids.at[c, :, theirs], m_s.at[k], m_r.at[k], dev).wait_recv()

    mid_copy = rc(mids.at[c], mids.at[c], x_s.at[3], x_r.at[3], partner)

    @pl.when(c == 0)
    def _():
        mid_copy.start()

    for dz in range(nz):
        pass_on(dz, 1 - c).wait_recv()
    head_grad = dot(mids[c], wfull[...])
    normed = norm_s[...]
    grad_ret = inv_s[...] * (
        head_grad
        - jnp.mean(head_grad, axis=-1, keepdims=True)
        - normed * jnp.mean(head_grad * normed, axis=-1, keepdims=True)
    )
    start = jnp.exp(-rate * steps)
    back_state[c] = dot_2(
        queries, start * grad_ret, 0, 0
    )
    back_copy = rc(back_state.at[c], back_state.at[c], x_s.at[4], x_r.at[4], partner)
    ret_s[...] = grad_ret

    def partial_out(dz):
        wide_cols = pl.ds(pl.multiple_of(lax.rem(z + dz, nz) * LANES, LANES), LANES)
        return dot(mids[0, :, wide_cols], mixes[0], 0, 0) + dot(
            mids[1, :, wide_cols], mixes[1], 0, 0
        )

    def up_copy(s, side):
        at = (s, pl.ds(side * 32, 32))
        return rc(up_s.at[at], up_r.at[at], o_s.at[0, s, side], o_r.at[0, s, side], at_z(1))

    def dn_copy(s, side):
        at = (s, pl.ds(side * 32, 32))
        return rc(dn_s.at[at], dn_r.at[at], o_s.at[1, s, side], o_r.at[1, s, side], at_z(down))

    def sum_step(s):
        up = partial_out(far - s)
        if s < far - 1:
            dn = partial_out(nz - (far - 1 - s))
        for side in range(4):
            part = slice(side * 32, side * 32 + 32)
            whole = up[part]
            if s > 0:
                up_copy(s - 1, side).wait_recv()
                whole = whole + up_r[s - 1, part, :].astype(F32)
            up_s[s, part, :] = whole.astype(BF)
            up_copy(s, side).start()
            if s < far - 1:
                whole = dn[part]
                if s > 0:
                    dn_copy(s - 1, side).wait_recv()
                    whole = whole + dn_r[s - 1, part, :].astype(F32)
                dn_s[s, part, :] = whole.astype(BF)
                dn_copy(s, side).start()

    def query_part():
        grad = ret_s[...]
        high, low = split(grad)
        sgrad[...] = dot2(grad, vals, 1, 1) * mask
        c_high, c_low = split(carried[...])
        carry = dot(high, c_high, 1, 1) + dot(low, c_high, 1, 1) + dot(high, c_low, 1, 1)
        gq_ref[...] = (dot2(sgrad[...], keys) + enter * carry).astype(BF)

    def value_part():
        high, low = split(ret_s[...])
        s_high, s_low = split(scores[...])
        part_v[...] = dot(s_high, high, 0, 0) + dot(s_low, high, 0, 0) + dot(s_high, low, 0, 0)
        part_k[...] = dot2(sgrad[...], queries, 0, 0)

    future_copy = rc(future, future, x_s.at[5], x_r.at[5], partner)
    gow_copy = rc(gow_s, gow_s, x_s.at[6], x_r.at[6], partner)
    trail = jnp.exp(-rate * (LANES - steps))

    def last_products(ahead):
        gv_ref[...] = (part_v[...] + trail * dot_2(keys, ahead)).astype(BF)
        gk_ref[...] = ((part_k[...] + trail * dot_2(vals, ahead, 1, 1)) * scale).astype(BF)

    @pl.when(c == 1)
    def _():
        back_copy.start()
        rc(mixes.at[0], mixes.at[0], x_s.at[2], x_r.at[2], partner).wait_recv()
        rc(mids.at[0], mids.at[0], x_s.at[3], x_r.at[3], partner).wait_recv()
        sum_step(0)
        query_part()
        sum_step(1)
        value_part()
        for s in range(2, far):
            sum_step(s)
        total = partial_out(0)
        for side in range(4):
            part = slice(side * 32, side * 32 + 32)
            dn_copy(far - 2, side).wait_recv()
            up_copy(far - 1, side).wait_recv()
            whole = (
                total[part] + dn_r[far - 2, part, :].astype(F32) + up_r[far - 1, part, :].astype(F32)
            )
            if side < 2:
                gow_s[part, :] = whole
            else:
                gow_ref[side * 32 - 64 : side * 32 - 32, :] = whole
            if side == 1:
                gow_copy.start()
        future_copy.wait_recv()
        last_products(future[...].astype(F32))
        for s in range(far):
            for side in range(4):
                up_copy(s, side).wait_send()
                if s < far - 1:
                    dn_copy(s, side).wait_send()
        back_copy.wait_send()
        gow_copy.wait_send()

    @pl.when(c == 0)
    def _():
        rc(back_state.at[1], back_state.at[1], x_s.at[4], x_r.at[4], partner).wait_recv()
        whole_back[...] = (back_state[0] + block_decay * back_state[1]).astype(BF)
        exchange(whole_back, bslices, h_s.at[0], h_r.at[0], 16)
        query_part()
        exchanged(whole_back, bslices, h_s.at[0], h_r.at[0], 16)
        running = jnp.zeros((16, 512), F32)
        for e in range(nz - 1, -1, -1):
            bscanned[e * 16 : e * 16 + 16, :] = running.astype(BF)
            running = chip_decay * running + bslices[e * 16 : e * 16 + 16, :].astype(F32)
        exchange(bscanned, future, h_s.at[1], h_r.at[1], 16)
        value_part()
        exchanged(bscanned, future, h_s.at[1], h_r.at[1], 16)
        future_copy.start()
        last_products(back_state[1] + block_decay * future[...].astype(F32))
        gow_copy.wait_recv()
        gow_ref[...] = gow_s[...]
        exchange_sent(whole_back, bslices, h_s.at[0], h_r.at[0], 16)
        exchange_sent(bscanned, future, h_s.at[1], h_r.at[1], 16)
        mix_copy.wait_send()
        mid_copy.wait_send()
        future_copy.wait_send()

    for s in range(far):
        ring(0, s + 1).wait_send()
        if s < far - 1:
            ring(1, s + 1).wait_send()
    for dz in range(nz):
        pass_on(dz, c).wait_send()
    exchange_sent(half_state, slices, f_s.at[0], f_r.at[0])
    exchange_sent(scanned, entered.at[rows_here], f_s.at[1], f_r.at[1])
    state_copy.wait_send()
    carry_copy.wait_send()
    for dz in range(1, nz):
        rc(sbuf.at[mine], xs.at[c, t, mine], z_s.at[dz], z_r.at[dz], at_z(dz)).wait_send()
        rc(rsend.at[here], ret.at[here], r_s.at[dz], r_r.at[dz], at_z(dz)).wait_send()
    weight_copy.wait_send()
    grad_copy.wait_send()
    for da in range(1, 4):
        a_copy(da).wait_send()

    @pl.loop(0, 4)
    def _(i):
        for k in range(4):
            b_copy(i, k, t).wait_send()
            d_copy(i, k, c, t).wait_send()

    for k in range(1, 4):
        q_copy(k).wait_send()
        v_copy(k).wait_send()

    @pl.loop(1, 16)
    def _(k):
        dev = peer(k // 4, lax.rem(k, 4))
        rc(mids.at[c, :, cols], mids.at[c, :, cols], m_s.at[k], m_r.at[k], dev).wait_send()


def local(
    cotangent,
    stream,
    routes,
    route_weights,
    gate_proj,
    up_proj,
    down_proj,
    out_weight,
    queries,
    keys,
    values,
    decay_rate,
):
    nz = lax.axis_size("z")
    width = cotangent.shape[1]
    rows, kept = nz * PAIR, nz * SLOTS
    far = nz // 2
    any_ = pl.BlockSpec(memory_space=pl.ANY)
    vmem = pl.BlockSpec(memory_space=pltpu.VMEM)
    dma = pltpu.SemaphoreType.DMA
    shapes = (
        jax.ShapeDtypeStruct((width, LANES), BF),
        jax.ShapeDtypeStruct((width, LANES), BF),
        jax.ShapeDtypeStruct((LANES, width), BF),
        jax.ShapeDtypeStruct(out_weight.shape, F32),
        jax.ShapeDtypeStruct(queries.shape, BF),
        jax.ShapeDtypeStruct(keys.shape, BF),
        jax.ShapeDtypeStruct(values.shape, BF),
    )
    grads = pl.pallas_call(
        functools.partial(kernel, nz),
        out_shape=tuple(pltpu.VMEM(a.shape, a.dtype) for a in shapes),
        in_specs=[vmem, vmem]
        + [any_] * 6
        + [vmem, vmem, vmem, pl.BlockSpec(memory_space=pltpu.SMEM)],
        out_specs=(vmem,) * 7,
        scratch_shapes=[
            pltpu.VMEM((2, width, 2 * LANES), BF),
            pltpu.VMEM((LANES, width), BF),
            pltpu.VMEM((LANES, LANES), BF),
            pltpu.VMEM((LANES, LANES), BF),
            pltpu.VMEM((rows, LANES), BF),
            pltpu.VMEM((2, 16, rows, LANES), BF),
            pltpu.VMEM((2, rows, 3 * LANES), F32),
            pltpu.VMEM((2, rows, 3 * LANES), BF),
            pltpu.VMEM((2, 3 * LANES, rows), BF),
            pltpu.VMEM((kept, 2 * LANES), BF),
            pltpu.VMEM((kept, 2 * LANES), BF),
            pltpu.VMEM((kept, 2 * LANES), BF),
            pltpu.VMEM((3, 4, kept, LANES), BF),
            pltpu.VMEM((4, kept, LANES), F32),
            pltpu.VMEM((3, 4, kept, LANES), BF),
            pltpu.VMEM((3, kept, LANES), BF),
            pltpu.VMEM((kept, LANES), F32),
            pltpu.VMEM((3, kept, LANES), BF),
            pltpu.VMEM((nz * BACK, LANES), BF),
            pltpu.VMEM((nz * BACK, LANES), BF),
            pltpu.VMEM((2, LANES, width), BF),
            pltpu.VMEM((width, 512), BF),
            pltpu.VMEM((2, 256, 512), F32),
            pltpu.VMEM((128, 512), F32),
            pltpu.VMEM((128, 512), F32),
            pltpu.VMEM((128, 512), BF),
            pltpu.VMEM((256, 512), F32),
            pltpu.VMEM((2, LANES, 512), BF),
            pltpu.VMEM((LANES, LANES), F32),
            pltpu.VMEM((LANES, 512), F32),
            pltpu.VMEM((LANES, 1), F32),
            pltpu.VMEM((2, 256, 512), F32),
            pltpu.VMEM((256, 512), BF),
            pltpu.VMEM((256, 512), BF),
            pltpu.VMEM((256, 512), BF),
            pltpu.VMEM((256, 512), BF),
            pltpu.VMEM((far, LANES, 512), BF),
            pltpu.VMEM((far, LANES, 512), BF),
            pltpu.VMEM((far - 1, LANES, 512), BF),
            pltpu.VMEM((far - 1, LANES, 512), BF),
            pltpu.VMEM((LANES, 512), F32),
            pltpu.VMEM((LANES, 256), F32),
            pltpu.VMEM((LANES, 512), F32),
            pltpu.VMEM((LANES, LANES), F32),
            pltpu.VMEM((64, 512), F32),
            pltpu.VMEM((256, 512), BF),
            dma((8,)),
            dma((nz,)),
            dma((nz,)),
            dma,
            dma,
            dma((4,)),
            dma((4,)),
            dma((4, 4)),
            dma((4, 4)),
            dma((4, 4)),
            dma((4, 4)),
            dma,
            dma,
            dma((3,)),
            dma((3,)),
            dma((3,)),
            dma((3,)),
            dma((nz,)),
            dma((nz,)),
            dma((16,)),
            dma((16,)),
            dma((2, far + 1)),
            dma((2, far + 1)),
            dma((nz,)),
            dma((nz,)),
            dma((7,)),
            dma((7,)),
            dma((2, nz)),
            dma((2, nz)),
            dma((2, nz)),
            dma((2, nz)),
            dma((2, far, 4)),
            dma((2, far, 4)),
        ],
        compiler_params=pltpu.CompilerParams(
            collective_id=0, has_side_effects=True, vmem_limit_bytes=58 * 2**20
        ),
        name="layer_backward",
    )(
        routes.T,
        route_weights,
        cotangent,
        stream,
        gate_proj[0],
        up_proj[0],
        down_proj[0],
        out_weight,
        queries,
        keys,
        values,
        decay_rate,
    )
    return tuple(g[None] for g in grads[:3]) + tuple(grads[3:])


def solution(mesh):
    blocks, heads = mesh.devices.shape
    split = Mesh(mesh.devices.reshape(blocks // 2, 2, 4, heads // 4), EVERY)
    tokens = P(SP, None)
    tiles = P(SP, TP)
    in_specs = (
        tokens,
        tokens,
        tokens,
        tokens,
        P(SP, None, TP),
        P(SP, None, TP),
        P(SP, TP, None),
        tiles,
        tiles,
        tiles,
        tiles,
        P(TP),
    )
    out_specs = (
        P(SP, None, TP),
        P(SP, None, TP),
        P(SP, TP, None),
        tiles,
        tiles,
        tiles,
        tiles,
    )
    return jax.shard_map(local, mesh=split, in_specs=in_specs, out_specs=out_specs, check_vma=False)
```

```python
import functools

import jax
import jax.numpy as jnp
from jax import lax
from jax.experimental import pallas as pl
from jax.experimental.pallas import tpu as pltpu
from jax.sharding import Mesh
from jax.sharding import PartitionSpec as P

SP = ("z", "c")
TP = ("y", "x")
EVERY = ("z", "c", "y", "x")
NORM_EPS = 1.0
SLOTS = 20
PAIR = 2 * SLOTS
BACK = 24
LANES = 128
BF = jnp.bfloat16
F32 = jnp.float32
MESH = pl.DeviceIdType.MESH


def dot(a, b, left=1, right=0):
    return lax.dot_general(a, b, (((left,), (right,)), ((), ())), preferred_element_type=F32)


def iota(shape, dim):
    return lax.broadcasted_iota(jnp.int32, shape, dim)


def kernel(
    nz,
    routes_ref,
    weights_ref,
    cot_hbm,
    stream_hbm,
    gate_hbm,
    up_hbm,
    down_hbm,
    out_weight_hbm,
    q_ref,
    k_ref,
    v_ref,
    rate_ref,
    gg_ref,
    gu_ref,
    gd_ref,
    gow_ref,
    gq_ref,
    gk_ref,
    gv_ref,
    wcat,
    down_v,
    cot_s,
    str_s,
    sbuf,
    xs,
    acc,
    wide,
    wide_t,
    gsend,
    gown,
    gpart,
    pbuf,
    pown,
    qbuf,
    tsum,
    town,
    vbuf,
    rsend,
    ret,
    mids,
    wfull,
    state,
    half_state,
    slices,
    scanned,
    carried,
    mixes,
    scores,
    norm_s,
    inv_s,
    back_state,
    whole_back,
    bslices,
    bscanned,
    future,
    up_s,
    up_r,
    dn_s,
    dn_r,
    part_v,
    part_k,
    ret_s,
    sgrad,
    gow_s,
    entered,
    loc,
    z_s,
    z_r,
    w_s,
    w_r,
    a_s,
    a_r,
    b_s,
    b_r,
    d_s,
    d_r,
    g_s,
    g_r,
    q_s,
    q_r,
    v_s,
    v_r,
    r_s,
    r_r,
    m_s,
    m_r,
    wr_s,
    wr_r,
    wd_s,
    wd_r,
    x_s,
    x_r,
    f_s,
    f_r,
    h_s,
    h_r,
    o_s,
    o_r,
):
    z, c, y, x = (lax.axis_index(a) for a in EVERY)
    rows = nz * PAIR
    half = rows // 2
    kept = nz * SLOTS
    t = y * 4 + x

    def peer(da, db):
        py = lax.rem(y + (1 - c) * da + c * db, 4)
        px = lax.rem(x + c * da + (1 - c) * db, 4)
        return (z, c, py, px)

    def tid(da, db):
        _, _, py, px = peer(da, db)
        return py * 4 + px

    def other_tid(da, db):
        py = lax.rem(y + c * da + (1 - c) * db, 4)
        px = lax.rem(x + (1 - c) * da + c * db, 4)
        return py * 4 + px

    def at_z(dz):
        return (lax.rem(z + dz, nz), c, y, x)

    partner = (z, 1 - c, y, x)

    def rc(src, dst, ss, rs, dev):
        return pltpu.make_async_remote_copy(
            src_ref=src, dst_ref=dst, send_sem=ss, recv_sem=rs, device_id=dev, device_id_type=MESH
        )

    def at_other(dz):
        return (lax.rem(z + dz, nz), 1 - c, y, x)

    def w_rows(dz, core):
        return pl.ds(pl.multiple_of((lax.rem(z + dz, nz) * 2 + core) * 64, 64), 64)

    rate = rate_ref[0]
    down = nz - 1

    def ring(way, s):
        dz = (nz - s + 1) if way == 0 else (s - 1)
        ref = wfull.at[w_rows(dz, c)]
        return rc(ref, ref, wr_s.at[way, s], wr_r.at[way, s], at_z(1 if way == 0 else down))

    def ring_got(way, s):
        dz = nz - s if way == 0 else s
        ref = wfull.at[w_rows(dz, c)]
        return rc(ref, ref, wr_s.at[way, s], wr_r.at[way, s], at_z(1 if way == 0 else down))

    def pass_on(dz, core):
        ref = wfull.at[w_rows(dz, core)]
        return rc(ref, ref, wd_s.at[dz], wd_r.at[dz], partner)

    far = nz // 2

    def ring_step(s):
        ring_got(0, s).wait_recv()
        if s < far:
            ring(0, s + 1).start()
        pass_on(nz - s, c).start()
        if s < far:
            ring_got(1, s).wait_recv()
            if s < far - 1:
                ring(1, s + 1).start()
            pass_on(s, c).start()

    barrier = pltpu.get_barrier_semaphore()

    @pl.loop(1, nz)
    def _(dz):
        pl.semaphore_signal(barrier, inc=1, device_id=at_z(dz), device_id_type=MESH)

    @pl.loop(1, 16)
    def _(k):
        pl.semaphore_signal(
            barrier, inc=1, device_id=peer(k // 4, lax.rem(k, 4)), device_id_type=MESH
        )

    pl.semaphore_signal(barrier, inc=1, device_id=partner, device_id_type=MESH)

    cols = pl.ds(pl.multiple_of(t * LANES, LANES), LANES)
    local = [
        pltpu.make_async_copy(cot_hbm.at[:, cols], cot_s, loc.at[0]),
        pltpu.make_async_copy(stream_hbm.at[:, cols], str_s, loc.at[1]),
        pltpu.make_async_copy(gate_hbm, wcat.at[0, :, pl.ds(0, LANES)], loc.at[2]),
        pltpu.make_async_copy(up_hbm, wcat.at[0, :, pl.ds(LANES, LANES)], loc.at[3]),
        pltpu.make_async_copy(down_hbm, down_v, loc.at[4]),
        pltpu.make_async_copy(out_weight_hbm, wfull.at[w_rows(0, c)], loc.at[7]),
    ]
    for copy in local:
        copy.start()

    experts = iota((nz, LANES), 0)
    named = [(experts == routes_ref[k : k + 1, :]).astype(F32) for k in range(2)]
    before = (iota((LANES, LANES), 0) < iota((LANES, LANES), 1)).astype(BF)
    count = dot((named[0] + named[1]).astype(BF), before)
    rank = [
        jnp.sum(named[k] * count, axis=0, keepdims=True).astype(jnp.int32) for k in range(2)
    ]
    slot = [routes_ref[k : k + 1, :] * PAIR + rank[k] for k in range(2)]
    places = iota((rows, LANES), 0)
    acc[...] = jnp.zeros_like(acc)
    local[0].wait()
    local[1].wait()
    cot = cot_s[...].astype(F32)
    packed = dot(
        jnp.logical_or(places == slot[0] + SLOTS, places == slot[1] + SLOTS).astype(F32).astype(BF),
        str_s[...],
    )
    same = (iota((LANES, LANES), 0) == iota((LANES, LANES), 1)).astype(F32).astype(BF)
    top = weights_ref[...].astype(BF)
    rest = weights_ref[...] - top.astype(F32)
    mid = rest.astype(BF)
    low = (rest - mid.astype(F32)).astype(BF)
    columns = dot(same, top, 1, 1) + dot(same, mid, 1, 1) + dot(same, low, 1, 1)
    for k in range(2):
        scaled = (columns[:, k : k + 1] * cot).astype(BF)
        packed = packed + dot((places == slot[k]).astype(F32).astype(BF), scaled)
    sbuf[...] = packed.astype(BF)

    pl.semaphore_wait(barrier, nz - 1 + 15 + 1)

    mine = pl.ds(pl.multiple_of(z * PAIR, 8), PAIR)
    for k in range(1, nz):
        dz = nz // 2 + (k // 2 if k % 2 == 0 else -(k // 2))
        there = pl.ds(pl.multiple_of(lax.rem(z + dz, nz) * PAIR, 8), PAIR)
        rc(sbuf.at[there], xs.at[c, t, mine], z_s.at[dz], z_r.at[dz], at_z(dz)).start()
    own = pltpu.make_async_copy(sbuf.at[mine], xs.at[c, t, mine], loc.at[5])
    own.start()
    steps = iota((LANES, 1), 0).astype(F32)
    scale = k_ref.shape[1] ** -0.5
    block_decay = jnp.exp(-rate * jnp.full((1, 512), float(LANES), F32))
    chip_decay = jnp.exp(-rate * jnp.full((1, 512), 2.0 * LANES, F32))
    keys = (k_ref[...].astype(F32) * scale).astype(BF)
    vals = v_ref[...]

    def split(a):
        high = a.astype(BF)
        return high, (a - high.astype(F32)).astype(BF)

    def dot2(a, b, left=1, right=0):
        high, low = split(a)
        return dot(high, b, left, right) + dot(low, b, left, right)

    def dot_2(a, b, left=1, right=0):
        high, low = split(b)
        return dot(a, high, left, right) + dot(a, low, left, right)

    leave = jnp.exp(-rate * (LANES - 1.0 - steps))
    state[c] = dot2(keys.astype(F32) * leave, vals, 0, 0)
    state_copy = rc(state.at[c], state.at[c], x_s.at[0], x_r.at[0], partner)
    state_copy.start()
    local[5].wait()
    ring(0, 1).start()
    ring(1, 1).start()
    pass_on(0, c).start()
    local[2].wait()
    local[3].wait()
    weight_copy = rc(wcat.at[0], wcat.at[1], w_s, w_r, partner)
    weight_copy.start()
    local[4].wait()
    own.wait()
    for dz in range(1, nz):
        here = pl.ds(pl.multiple_of(lax.rem(z + nz - dz, nz) * PAIR, 8), PAIR)
        rc(sbuf.at[mine], xs.at[c, t, here], z_s.at[dz], z_r.at[dz], at_z(dz)).wait_recv()

    def product(core, pieces):
        deep = [pl.ds(pl.multiple_of(piece * LANES, LANES), LANES) for piece in pieces]
        a = jnp.concatenate([xs[core, piece] for piece in pieces], axis=1)
        acc[core, :, 0:256] += dot(a, jnp.concatenate([wcat[0, d, :] for d in deep], axis=0))
        acc[core, :, 256:384] += dot(a, jnp.concatenate([down_v[:, d] for d in deep], axis=1), 1, 1)

    first = pl.ds(0, half)
    last = pl.ds(half, half)

    def a_copy(da):
        ref = xs.at[c, t]
        return rc(ref, ref, a_s.at[da], a_r.at[da], peer(da, 0))

    def a_got(da):
        ref = xs.at[c, tid(4 - da, 0)]
        rc(ref, ref, a_s.at[da], a_r.at[da], peer(da, 0)).wait_recv()

    def b_copy(i, k, piece):
        part = (slice(None), slice(None), first, last)[k]
        ref = xs.at[c, piece] if k < 2 else xs.at[c, piece, part]
        return rc(ref, ref, b_s.at[i, k], b_r.at[i, k], peer(0, 1 if k % 2 == 0 else 3))

    def d_copy(i, j, core, piece):
        ref = xs.at[core, piece]
        return rc(ref, ref, d_s.at[i, j], d_r.at[i, j], partner)

    def spread(i, piece):
        b_copy(i, 0, piece).start()
        b_copy(i, 1, piece).start()
        d_copy(i, 0, c, piece).start()

    for da in (1, 3, 2):
        a_copy(da).start()
    spread(0, t)
    ring_step(1)
    for i, da in ((1, 1), (2, 3), (3, 2)):
        a_got(da)
        spread(i, tid(4 - da, 0))
    ring_step(2)

    rows_here = pl.ds(pl.multiple_of(c * 128, 128), 128)
    rows_there = pl.ds(pl.multiple_of((1 - c) * 128, 128), 128)

    def slice_of(dz, n):
        return pl.ds(pl.multiple_of(lax.rem(z + dz, nz) * n, 8), n)

    def exchange(src, dst, ss, rs, n=8):
        for k in range(1, nz):
            dz = nz // 2 + (k // 2 if k % 2 == 0 else -(k // 2))
            rc(src.at[slice_of(dz, n)], dst.at[slice_of(0, n)], ss.at[dz], rs.at[dz], at_z(dz)).start()
        mine_copy = pltpu.make_async_copy(src.at[slice_of(0, n)], dst.at[slice_of(0, n)], ss.at[0])
        mine_copy.start()

    def exchanged(src, dst, ss, rs, n=8):
        pltpu.make_async_copy(src.at[slice_of(0, n)], dst.at[slice_of(0, n)], ss.at[0]).wait()
        for dz in range(1, nz):
            rc(
                src.at[slice_of(0, n)], dst.at[slice_of(nz - dz, n)], ss.at[dz], rs.at[dz], at_z(dz)
            ).wait_recv()

    def exchange_sent(src, dst, ss, rs, n=8):
        for dz in range(1, nz):
            rc(src.at[slice_of(0, n)], dst.at[slice_of(0, n)], ss.at[dz], rs.at[dz], at_z(dz)).wait_send()

    rc(state.at[1 - c], state.at[1 - c], x_s.at[0], x_r.at[0], partner).wait_recv()
    half_state[...] = (block_decay * state[0, rows_here, :] + state[1, rows_here, :]).astype(BF)

    def offset(i):
        return (lax.rem(i + 1, 3) + 1) * jnp.minimum(i, 1)

    def near_from_partner(i):
        da = offset(i)
        pieces = [other_tid(da, db) for db in (0, 3, 1)]
        for j in range(3):
            d_copy(i, j, 1 - c, pieces[j]).wait_recv()
        product(1 - c, pieces)

    @pl.loop(0, 4)
    def _(i):
        da = offset(i)
        left, right = tid(da, 3), tid(da, 1)
        b_copy(i, 0, left).wait_recv()
        b_copy(i, 2, left).start()
        d_copy(i, 1, c, left).start()
        b_copy(i, 1, right).wait_recv()
        b_copy(i, 3, right).start()
        d_copy(i, 2, c, right).start()
        product(c, [tid(da, 0), left, right])

        @pl.when(i > 0)
        def _():
            near_from_partner(i - 1)

    ring_step(3)
    near_from_partner(3)
    fars = [tid(da, 2) for da in (0, 3, 1, 2)]
    for i in range(4):
        b_copy(i, 2, fars[i]).wait_recv()
        b_copy(i, 3, fars[i]).wait_recv()
        d_copy(i, 3, c, fars[i]).start()
    product(c, fars)
    ring_step(4)
    fars = [other_tid(da, 2) for da in (0, 3, 1, 2)]
    for i in range(4):
        d_copy(i, 3, 1 - c, fars[i]).wait_recv()
    product(1 - c, fars)
    exchange(half_state, slices, f_s.at[0], f_r.at[0])

    @pl.loop(0, 2 * rows // 80)
    def _(k):
        core = k // (rows // 80)
        at = pl.ds(pl.multiple_of(lax.rem(k, rows // 80) * 80, 8), 80)
        lane_row = iota((80, LANES), 0)
        is_in = jnp.logical_or(
            jnp.logical_and(lane_row >= 20, lane_row < 40), lane_row >= 60
        )
        pre_gate = acc[core, at, 0:128]
        pre_up = acc[core, at, 128:256]
        grad_hidden = pltpu.roll(acc[core, at, 256:384], 20, axis=0)
        gate = jax.nn.sigmoid(pre_gate)
        active = pre_gate * gate
        hidden = active * pre_up
        grad_gate = grad_hidden * pre_up * (gate * (1.0 + pre_gate * (1.0 - gate)))
        grad_up = grad_hidden * active
        wide[core, at, 0:128] = jnp.where(is_in, grad_gate, 0.0).astype(BF)
        wide[core, at, 128:256] = jnp.where(is_in, grad_up, 0.0).astype(BF)
        wide[core, at, 256:384] = jnp.where(is_in, 0.0, pltpu.roll(hidden, 60, axis=0)).astype(BF)

    low = iota((kept, rows), 0)
    pick = (iota((kept, rows), 1) == low + SLOTS * ((low * 3277) // 65536) + SLOTS)
    pick = pick.astype(F32).astype(BF)
    gsend[...] = dot(pick, wide[1 - c, :, 0:256]).astype(BF)
    grad_copy = rc(gsend, gpart, g_s, g_r, partner)
    grad_copy.start()
    gown[...] = dot(pick, wide[c, :, 0:256]).astype(BF)
    weight_copy.wait_recv()
    grad_copy.wait_recv()

    def partial_in(pieces):
        deep = [pl.ds(pl.multiple_of(piece * LANES, LANES), LANES) for piece in pieces]
        own_w, their_w = (jnp.concatenate([wcat[k, d, :] for d in deep], axis=0) for k in range(2))
        return dot(gown[...], own_w, 1, 1) + dot(gpart[...], their_w, 1, 1)

    def q_copy(da):
        return rc(pbuf.at[da - 1], qbuf.at[da - 1], q_s.at[da - 1], q_r.at[da - 1], peer(da, 0))

    for da in (2, 1, 3):

        for db in (0, 2):
            both = partial_in((tid(da, db), tid(da, db + 1))).astype(BF)
            pbuf[da - 1, db] = both[:, 0:LANES]
            pbuf[da - 1, db + 1] = both[:, LANES:]

        q_copy(da).start()

    for db in (0, 2):
        both = partial_in((tid(0, db), tid(0, db + 1)))
        pown[db] = both[:, 0:LANES]
        pown[db + 1] = both[:, LANES:]

    ring_step(5)

    for core in range(2):
        wide_t[core] = wide[core].T

    def weight_grads(pair):
        deep = pl.ds(pl.multiple_of(pair * 2 * LANES, 2 * LANES), 2 * LANES)
        total = 0.0
        for core in range(2):
            both = jnp.concatenate([xs[core, pair * 2], xs[core, pair * 2 + 1]], axis=1)
            total = total + dot(wide_t[core], both)
        gd_ref[:, deep] = total[256:384].astype(BF)
        gg_ref[deep, :] = total[0:128].T.astype(BF)
        gu_ref[deep, :] = total[128:256].T.astype(BF)

    @pl.loop(0, 4)
    def _(pair):
        weight_grads(pair)

    @pl.loop(4, 8)
    def _(pair):
        weight_grads(pair)

    ring_step(6)
    exchanged(half_state, slices, f_s.at[0], f_r.at[0])
    running = jnp.zeros((8, 512), F32)
    for e in range(nz):
        scanned[e * 8 : e * 8 + 8, :] = running.astype(BF)
        running = chip_decay * running + slices[e * 8 : e * 8 + 8, :].astype(F32)
    exchange(scanned, entered.at[rows_here], f_s.at[1], f_r.at[1])
    for da in (1, 3, 2):
        q_copy(da).wait_recv()

    def v_copy(db):
        return rc(tsum.at[db - 1], vbuf.at[db - 1], v_s.at[db - 1], v_r.at[db - 1], peer(0, db))

    for db in (2, 1, 3):
        whole = pown[db]
        for da in range(3):
            whole = whole + qbuf[da, db].astype(F32)
        tsum[db - 1] = whole.astype(BF)
        v_copy(db).start()
    whole = pown[0]
    for da in range(3):
        whole = whole + qbuf[da, 0].astype(F32)
    town[...] = whole
    ring_step(7)
    for db in (1, 3, 2):
        v_copy(db).wait_recv()
    whole = town[...]
    for db in range(3):
        whole = whole + vbuf[db].astype(F32)
    low = iota((nz * BACK, kept), 0)
    block = (low * 2731) // 65536
    spreadm = jnp.logical_and(
        iota((nz * BACK, kept), 1) == low - (BACK - SLOTS) * block, low - BACK * block < SLOTS
    )
    rsend[...] = dot(spreadm.astype(F32).astype(BF), whole.astype(BF)).astype(BF)

    here = pl.ds(pl.multiple_of(z * BACK, 8), BACK)
    for k in range(1, nz):
        dz = nz // 2 + (k // 2 if k % 2 == 0 else -(k // 2))
        there = pl.ds(pl.multiple_of(lax.rem(z + dz, nz) * BACK, 8), BACK)
        rc(rsend.at[there], ret.at[here], r_s.at[dz], r_r.at[dz], at_z(dz)).start()
    own = pltpu.make_async_copy(rsend.at[here], ret.at[here], loc.at[6])
    own.start()
    places = iota((nz * BACK, LANES), 0)
    take = jnp.logical_or(
        places == routes_ref[0:1, :] * BACK + rank[0], places == routes_ref[1:2, :] * BACK + rank[1]
    )
    take = take.astype(F32).astype(BF)
    own.wait()
    exchanged(scanned, entered.at[rows_here], f_s.at[1], f_r.at[1])
    carry_copy = rc(entered.at[rows_here], entered.at[rows_here], x_s.at[1], x_r.at[1], partner)
    carry_copy.start()

    distance = iota((LANES, LANES), 0) - iota((LANES, LANES), 1)
    mask = jnp.where(
        distance >= 0, jnp.exp(-rate * jnp.maximum(distance, 0).astype(F32)), 0.0
    )
    enter = jnp.exp(-rate * (steps + 1.0))
    queries = q_ref[...]
    rc(entered.at[rows_there], entered.at[rows_there], x_s.at[1], x_r.at[1], partner).wait_recv()

    inside = entered[...].astype(F32)
    carried[...] = jnp.where(c == 1, block_decay * inside + state[0], inside)
    scores[...] = dot(queries, keys, 1, 1) * mask
    retained = dot2(scores[...], vals) + enter * dot_2(queries, carried[...])
    centered = retained - jnp.mean(retained, axis=-1, keepdims=True)
    inv = lax.rsqrt(jnp.mean(centered * centered, axis=-1, keepdims=True) + NORM_EPS)
    norm_s[...] = centered * inv
    inv_s[...] = inv
    mixes[c] = norm_s[...].astype(BF)
    mix_copy = rc(mixes.at[c], mixes.at[c], x_s.at[2], x_r.at[2], partner)

    @pl.when(c == 0)
    def _():
        mix_copy.start()

    ring_step(8)
    for dz in range(1, nz):
        there = pl.ds(pl.multiple_of(lax.rem(z + nz - dz, nz) * BACK, 8), BACK)
        rc(rsend.at[here], ret.at[there], r_s.at[dz], r_r.at[dz], at_z(dz)).wait_recv()
    mids[c, :, cols] = (cot_s[...].astype(F32) + dot(take, ret[...], 0, 0)).astype(BF)

    @pl.loop(1, 16)
    def _(k):
        dev = peer(k // 4, lax.rem(k, 4))
        rc(mids.at[c, :, cols], mids.at[c, :, cols], m_s.at[k], m_r.at[k], dev).start()

    @pl.loop(1, 16)
    def _(k):
        back = tid(lax.rem(4 - k // 4, 4), lax.rem(4 - lax.rem(k, 4), 4))
        theirs = pl.ds(pl.multiple_of(back * LANES, LANES), LANES)
        dev = peer(k // 4, lax.rem(k, 4))
        rc(mids.at[c, :, cols], mids.at[c, :, theirs], m_s.at[k], m_r.at[k], dev).wait_recv()

    mid_copy = rc(mids.at[c], mids.at[c], x_s.at[3], x_r.at[3], partner)

    @pl.when(c == 0)
    def _():
        mid_copy.start()

    for dz in range(nz):
        pass_on(dz, 1 - c).wait_recv()
    head_grad = dot(mids[c], wfull[...])
    normed = norm_s[...]
    grad_ret = inv_s[...] * (
        head_grad
        - jnp.mean(head_grad, axis=-1, keepdims=True)
        - normed * jnp.mean(head_grad * normed, axis=-1, keepdims=True)
    )
    start = jnp.exp(-rate * steps)
    back_state[c] = dot_2(
        queries, start * grad_ret, 0, 0
    )
    back_copy = rc(back_state.at[c], back_state.at[c], x_s.at[4], x_r.at[4], partner)
    ret_s[...] = grad_ret

    def partial_out(dz):
        wide_cols = pl.ds(pl.multiple_of(lax.rem(z + dz, nz) * LANES, LANES), LANES)
        return dot(mids[0, :, wide_cols], mixes[0], 0, 0) + dot(
            mids[1, :, wide_cols], mixes[1], 0, 0
        )

    def up_copy(s, side):
        at = (s, pl.ds(side * 32, 32))
        return rc(up_s.at[at], up_r.at[at], o_s.at[0, s, side], o_r.at[0, s, side], at_z(1))

    def dn_copy(s, side):
        at = (s, pl.ds(side * 32, 32))
        return rc(dn_s.at[at], dn_r.at[at], o_s.at[1, s, side], o_r.at[1, s, side], at_z(down))

    def sum_step(s):
        up = partial_out(far - s)
        if s < far - 1:
            dn = partial_out(nz - (far - 1 - s))
        for side in range(4):
            part = slice(side * 32, side * 32 + 32)
            whole = up[part]
            if s > 0:
                up_copy(s - 1, side).wait_recv()
                whole = whole + up_r[s - 1, part, :].astype(F32)
            up_s[s, part, :] = whole.astype(BF)
            up_copy(s, side).start()
            if s < far - 1:
                whole = dn[part]
                if s > 0:
                    dn_copy(s - 1, side).wait_recv()
                    whole = whole + dn_r[s - 1, part, :].astype(F32)
                dn_s[s, part, :] = whole.astype(BF)
                dn_copy(s, side).start()

    def query_part():
        grad = ret_s[...]
        high, low = split(grad)
        sgrad[...] = dot2(grad, vals, 1, 1) * mask
        c_high, c_low = split(carried[...])
        carry = dot(high, c_high, 1, 1) + dot(low, c_high, 1, 1) + dot(high, c_low, 1, 1)
        gq_ref[...] = (dot2(sgrad[...], keys) + enter * carry).astype(BF)

    def value_part():
        high, low = split(ret_s[...])
        s_high, s_low = split(scores[...])
        part_v[...] = dot(s_high, high, 0, 0) + dot(s_low, high, 0, 0) + dot(s_high, low, 0, 0)
        part_k[...] = dot2(sgrad[...], queries, 0, 0)

    future_copy = rc(future, future, x_s.at[5], x_r.at[5], partner)
    gow_copy = rc(gow_s, gow_s, x_s.at[6], x_r.at[6], partner)
    trail = jnp.exp(-rate * (LANES - steps))

    def last_products(ahead):
        gv_ref[...] = (part_v[...] + trail * dot_2(keys, ahead)).astype(BF)
        gk_ref[...] = ((part_k[...] + trail * dot_2(vals, ahead, 1, 1)) * scale).astype(BF)

    @pl.when(c == 1)
    def _():
        back_copy.start()
        rc(mixes.at[0], mixes.at[0], x_s.at[2], x_r.at[2], partner).wait_recv()
        rc(mids.at[0], mids.at[0], x_s.at[3], x_r.at[3], partner).wait_recv()
        sum_step(0)
        query_part()
        sum_step(1)
        value_part()
        for s in range(2, far):
            sum_step(s)
        total = partial_out(0)
        for side in range(4):
            part = slice(side * 32, side * 32 + 32)
            dn_copy(far - 2, side).wait_recv()
            up_copy(far - 1, side).wait_recv()
            whole = (
                total[part] + dn_r[far - 2, part, :].astype(F32) + up_r[far - 1, part, :].astype(F32)
            )
            if side < 2:
                gow_s[part, :] = whole
            else:
                gow_ref[side * 32 - 64 : side * 32 - 32, :] = whole
            if side == 1:
                gow_copy.start()
        future_copy.wait_recv()
        last_products(future[...].astype(F32))
        for s in range(far):
            for side in range(4):
                up_copy(s, side).wait_send()
                if s < far - 1:
                    dn_copy(s, side).wait_send()
        back_copy.wait_send()
        gow_copy.wait_send()

    @pl.when(c == 0)
    def _():
        rc(back_state.at[1], back_state.at[1], x_s.at[4], x_r.at[4], partner).wait_recv()
        whole_back[...] = (back_state[0] + block_decay * back_state[1]).astype(BF)
        exchange(whole_back, bslices, h_s.at[0], h_r.at[0], 16)
        query_part()
        exchanged(whole_back, bslices, h_s.at[0], h_r.at[0], 16)
        running = jnp.zeros((16, 512), F32)
        for e in range(nz - 1, -1, -1):
            bscanned[e * 16 : e * 16 + 16, :] = running.astype(BF)
            running = chip_decay * running + bslices[e * 16 : e * 16 + 16, :].astype(F32)
        exchange(bscanned, future, h_s.at[1], h_r.at[1], 16)
        value_part()
        exchanged(bscanned, future, h_s.at[1], h_r.at[1], 16)
        future_copy.start()
        last_products(back_state[1] + block_decay * future[...].astype(F32))
        gow_copy.wait_recv()
        gow_ref[...] = gow_s[...]
        exchange_sent(whole_back, bslices, h_s.at[0], h_r.at[0], 16)
        exchange_sent(bscanned, future, h_s.at[1], h_r.at[1], 16)
        mix_copy.wait_send()
        mid_copy.wait_send()
        future_copy.wait_send()

    for s in range(far):
        ring(0, s + 1).wait_send()
        if s < far - 1:
            ring(1, s + 1).wait_send()
    for dz in range(nz):
        pass_on(dz, c).wait_send()
    exchange_sent(half_state, slices, f_s.at[0], f_r.at[0])
    exchange_sent(scanned, entered.at[rows_here], f_s.at[1], f_r.at[1])
    state_copy.wait_send()
    carry_copy.wait_send()
    for dz in range(1, nz):
        rc(sbuf.at[mine], xs.at[c, t, mine], z_s.at[dz], z_r.at[dz], at_z(dz)).wait_send()
        rc(rsend.at[here], ret.at[here], r_s.at[dz], r_r.at[dz], at_z(dz)).wait_send()
    weight_copy.wait_send()
    grad_copy.wait_send()
    for da in range(1, 4):
        a_copy(da).wait_send()

    @pl.loop(0, 4)
    def _(i):
        for k in range(4):
            b_copy(i, k, t).wait_send()
            d_copy(i, k, c, t).wait_send()

    for k in range(1, 4):
        q_copy(k).wait_send()
        v_copy(k).wait_send()

    @pl.loop(1, 16)
    def _(k):
        dev = peer(k // 4, lax.rem(k, 4))
        rc(mids.at[c, :, cols], mids.at[c, :, cols], m_s.at[k], m_r.at[k], dev).wait_send()


def put_out(*refs):
    copies = [pltpu.make_async_copy(refs[k], refs[7 + k], refs[14].at[k]) for k in range(7)]
    for copy in copies:
        copy.start()
    for copy in copies:
        copy.wait()


def local(
    cotangent,
    stream,
    routes,
    route_weights,
    gate_proj,
    up_proj,
    down_proj,
    out_weight,
    queries,
    keys,
    values,
    decay_rate,
):
    nz = lax.axis_size("z")
    width = cotangent.shape[1]
    rows, kept = nz * PAIR, nz * SLOTS
    far = nz // 2
    any_ = pl.BlockSpec(memory_space=pl.ANY)
    vmem = pl.BlockSpec(memory_space=pltpu.VMEM)
    dma = pltpu.SemaphoreType.DMA
    shapes = (
        jax.ShapeDtypeStruct((width, LANES), BF),
        jax.ShapeDtypeStruct((width, LANES), BF),
        jax.ShapeDtypeStruct((LANES, width), BF),
        jax.ShapeDtypeStruct(out_weight.shape, F32),
        jax.ShapeDtypeStruct(queries.shape, BF),
        jax.ShapeDtypeStruct(keys.shape, BF),
        jax.ShapeDtypeStruct(values.shape, BF),
    )
    grads = pl.pallas_call(
        functools.partial(kernel, nz),
        out_shape=tuple(pltpu.VMEM(a.shape, a.dtype) for a in shapes),
        in_specs=[vmem, vmem]
        + [any_] * 6
        + [vmem, vmem, vmem, pl.BlockSpec(memory_space=pltpu.SMEM)],
        out_specs=(vmem,) * 7,
        scratch_shapes=[
            pltpu.VMEM((2, width, 2 * LANES), BF),
            pltpu.VMEM((LANES, width), BF),
            pltpu.VMEM((LANES, LANES), BF),
            pltpu.VMEM((LANES, LANES), BF),
            pltpu.VMEM((rows, LANES), BF),
            pltpu.VMEM((2, 16, rows, LANES), BF),
            pltpu.VMEM((2, rows, 3 * LANES), F32),
            pltpu.VMEM((2, rows, 3 * LANES), BF),
            pltpu.VMEM((2, 3 * LANES, rows), BF),
            pltpu.VMEM((kept, 2 * LANES), BF),
            pltpu.VMEM((kept, 2 * LANES), BF),
            pltpu.VMEM((kept, 2 * LANES), BF),
            pltpu.VMEM((3, 4, kept, LANES), BF),
            pltpu.VMEM((4, kept, LANES), F32),
            pltpu.VMEM((3, 4, kept, LANES), BF),
            pltpu.VMEM((3, kept, LANES), BF),
            pltpu.VMEM((kept, LANES), F32),
            pltpu.VMEM((3, kept, LANES), BF),
            pltpu.VMEM((nz * BACK, LANES), BF),
            pltpu.VMEM((nz * BACK, LANES), BF),
            pltpu.VMEM((2, LANES, width), BF),
            pltpu.VMEM((width, 512), BF),
            pltpu.VMEM((2, 256, 512), F32),
            pltpu.VMEM((128, 512), BF),
            pltpu.VMEM((128, 512), BF),
            pltpu.VMEM((128, 512), BF),
            pltpu.VMEM((256, 512), F32),
            pltpu.VMEM((2, LANES, 512), BF),
            pltpu.VMEM((LANES, LANES), F32),
            pltpu.VMEM((LANES, 512), F32),
            pltpu.VMEM((LANES, 1), F32),
            pltpu.VMEM((2, 256, 512), F32),
            pltpu.VMEM((256, 512), BF),
            pltpu.VMEM((256, 512), BF),
            pltpu.VMEM((256, 512), BF),
            pltpu.VMEM((256, 512), BF),
            pltpu.VMEM((far, LANES, 512), BF),
            pltpu.VMEM((far, LANES, 512), BF),
            pltpu.VMEM((far - 1, LANES, 512), BF),
            pltpu.VMEM((far - 1, LANES, 512), BF),
            pltpu.VMEM((LANES, 512), F32),
            pltpu.VMEM((LANES, 256), F32),
            pltpu.VMEM((LANES, 512), F32),
            pltpu.VMEM((LANES, LANES), F32),
            pltpu.VMEM((64, 512), F32),
            pltpu.VMEM((256, 512), BF),
            dma((8,)),
            dma((nz,)),
            dma((nz,)),
            dma,
            dma,
            dma((4,)),
            dma((4,)),
            dma((4, 4)),
            dma((4, 4)),
            dma((4, 4)),
            dma((4, 4)),
            dma,
            dma,
            dma((3,)),
            dma((3,)),
            dma((3,)),
            dma((3,)),
            dma((nz,)),
            dma((nz,)),
            dma((16,)),
            dma((16,)),
            dma((2, far + 1)),
            dma((2, far + 1)),
            dma((nz,)),
            dma((nz,)),
            dma((7,)),
            dma((7,)),
            dma((2, nz)),
            dma((2, nz)),
            dma((2, nz)),
            dma((2, nz)),
            dma((2, far, 4)),
            dma((2, far, 4)),
        ],
        compiler_params=pltpu.CompilerParams(
            collective_id=0, has_side_effects=True, vmem_limit_bytes=58 * 2**20
        ),
        name="layer_backward",
    )(
        routes.T,
        route_weights.T,
        cotangent,
        stream,
        gate_proj[0],
        up_proj[0],
        down_proj[0],
        out_weight,
        queries,
        keys,
        values,
        decay_rate,
    )
    grads = pl.pallas_call(
        put_out,
        out_shape=shapes,
        in_specs=[any_] * 7,
        out_specs=(any_,) * 7,
        scratch_shapes=[dma((7,))],
        name="put_out",
    )(*(pltpu.with_memory_space_constraint(g, pltpu.VMEM) for g in grads))
    return tuple(g[None] for g in grads[:3]) + tuple(grads[3:])


def solution(mesh):
    blocks, heads = mesh.devices.shape
    split = Mesh(mesh.devices.reshape(blocks // 2, 2, 4, heads // 4), EVERY)
    tokens = P(SP, None)
    tiles = P(SP, TP)
    in_specs = (
        tokens,
        tokens,
        tokens,
        tokens,
        P(SP, None, TP),
        P(SP, None, TP),
        P(SP, TP, None),
        tiles,
        tiles,
        tiles,
        tiles,
        P(TP),
    )
    out_specs = (
        P(SP, None, TP),
        P(SP, None, TP),
        P(SP, TP, None),
        tiles,
        tiles,
        tiles,
        tiles,
    )
    return jax.shard_map(local, mesh=split, in_specs=in_specs, out_specs=out_specs, check_vma=False)
```
